128 devices in a mesh: fs: 16 (over z, x), tp: 8 (over y, core).
Axes of the slice: x: 4, y: 4, z: 4, core: 2. Of those that a mesh axis runs over, the one named last changes fastest.
Arguments:
- later_input: bfloat16 [12288, 2048], P('fs', 'tp'), may hold values from -6 to 6
- earlier_input: bfloat16 [12288, 2048], P('fs', 'tp'), may hold values from -6 to 6
- cotangent: bfloat16 [12288, 2048], P('fs', 'tp'), may hold values from -6 to 6
- up_weight: bfloat16 [2048, 8192], P('fs', 'tp'), may hold values from -0.125 to 0.125
- down_weight: bfloat16 [8192, 2048], P('tp', 'fs'), may hold values from -0.0625 to 0.0625
- up_running: float32 [2048, 8192], P('fs', 'tp'), may hold values from -6 to 6
- down_running: float32 [2048, 8192], P('fs', 'tp'), may hold values from -6 to 6
Outputs:
- later_output: bfloat16 [12288, 2048], P('fs', 'tp')
- later_preact: bfloat16 [12288, 8192], P('fs', 'tp')
- earlier_grad: bfloat16 [12288, 2048], P('fs', 'tp')
- up_running_out: float32 [2048, 8192], P('fs', 'tp')
- down_running_out: float32 [2048, 8192], P('fs', 'tp')
The draws below stay inside these ranges and needn't reach their ends.
All inputs are finite; a program needn't handle non-finite values.
Results may differ from the reference program's by a relative error of at most 0.014.
Values may be sent and summed in bfloat16 or wider, within the bound.
A program may use at most 128 MiB of HBM per device.

```python
import jax
import jax.numpy as jnp
from jax import lax

D = 2048
FF = 8192
TOKENS = 12288
N_TP = 8


def with_spikes(values, own_key, source, target, blocks, factor):
    def block_of(axis_at):
        return (jnp.arange(values.shape[axis_at]) // (values.shape[axis_at] // blocks)).reshape((-1,) + (1,) * (values.ndim - 1 - axis_at))

    near = jax.random.permutation(own_key, blocks)[block_of(target)]
    far = (block_of(target) + blocks // 2) % blocks
    return jnp.where((block_of(source) == near) | (block_of(source) == far), factor * values, values)


def steps_of(rng, shape, pieces, least, top_value):
    factor_of, own = 1.0, jax.random.fold_in(rng, 6)
    for position, blocks in pieces:
        steps = jnp.exp(jax.random.uniform(jax.random.fold_in(own, position), (blocks,), jnp.float32, least / len(pieces), top_value / len(pieces)))
        factor_of = factor_of * jnp.repeat(steps, shape[position] // blocks).reshape([-1 if axis == position else 1 for axis in range(len(shape))])
    return factor_of


def scatter_about(key, dims, scale, bound, split=(), kind=jnp.bfloat16):
    result = scale * jax.random.normal(key, dims, jnp.float32)
    if split:
        result = result * steps_of(key, dims, split, -0.22, 0.18)
    return jnp.clip(result, -bound, bound).astype(kind)


def heavy_noise(own_key, dims, scale, reach, split, heavy, held_as=jnp.bfloat16):
    drawn = scale * jax.random.normal(own_key, dims, jnp.float32)
    if split:
        drawn = drawn * steps_of(own_key, dims, split, -0.22, 0.18)
    return jnp.clip(with_spikes(drawn, jax.random.fold_in(own_key, 3), *heavy), -reach, reach).astype(held_as)


def setup_inputs(seed: int = 0) -> dict:
    splits = jax.random.split(jax.random.key(seed), 8)
    return {
        "later_input": scatter_about(splits[0], (TOKENS, D), 1.0, 6.0, ((0, 16), (1, 8))),
        "earlier_input": scatter_about(splits[1], (TOKENS, D), 1.0, 6.0, ((0, 16), (1, 8))),
        "cotangent": heavy_noise(splits[2], (TOKENS, D), 1.0, 6.0, ((0, 16), (1, 8)), (0, 1, 16, 2.0)),
        "up_weight": scatter_about(splits[3], (D, FF), D ** -0.5, 0.125, ((0, 16), (1, 8))),
        "down_weight": scatter_about(splits[4], (FF, D), FF ** -0.5, 0.0625, ((0, 8), (1, 16))),
        "up_running": scatter_about(splits[5], (D, FF), 1.0, 6.0, ((0, 16), (1, 8)), jnp.float32),
        "down_running": scatter_about(splits[6], (D, FF), 1.0, 6.0, ((0, 16), (1, 8)), jnp.float32),
    }


def block_sum(left, right):
    rows = left.shape[0]
    width = left.shape[1] // N_TP
    left_blocks = left.reshape(rows, N_TP, width).transpose(1, 0, 2)
    right_blocks = right.reshape(N_TP, width, right.shape[1])

    def step(total, pair):
        part = jnp.dot(pair[0], pair[1], preferred_element_type=jnp.float32).astype(jnp.bfloat16)
        part = lax.optimization_barrier(part)
        return total + part.astype(jnp.float32), None

    start = jnp.zeros((rows, right.shape[1]), jnp.float32)
    total, _ = lax.scan(step, start, (left_blocks, right_blocks))
    return total.astype(jnp.bfloat16)


def reference(later_input, earlier_input, cotangent, up_weight, down_weight, up_running, down_running):
    later_up = jnp.dot(later_input, up_weight, preferred_element_type=jnp.float32)
    later_preact = later_up.astype(jnp.bfloat16)
    later_hidden = jnp.square(jax.nn.relu(later_up)).astype(jnp.bfloat16)
    later_output = block_sum(later_hidden, down_weight)
    earlier_up = jnp.dot(earlier_input, up_weight, preferred_element_type=jnp.float32)
    earlier_hidden = jnp.square(jax.nn.relu(earlier_up)).astype(jnp.bfloat16)
    hidden_grad = jnp.dot(cotangent, down_weight.T, preferred_element_type=jnp.float32)
    up_grad = (2.0 * jax.nn.relu(earlier_up) * hidden_grad).astype(jnp.bfloat16)
    earlier_grad = block_sum(up_grad, up_weight.T)
    factor = float(TOKENS) ** -0.5
    up_running_out = up_running + jnp.dot(earlier_input.T, up_grad, preferred_element_type=jnp.float32) * factor
    down_running_out = down_running + jnp.dot(cotangent.T, earlier_hidden, preferred_element_type=jnp.float32) * factor
    return later_output, later_preact, earlier_grad, up_running_out, down_running_out
```

```python
import jax
import jax.numpy as jnp
from jax import lax
from jax.experimental import pallas as pl
from jax.experimental.pallas import tpu as pltpu
from jax.sharding import PartitionSpec as P

contract_last = (((1,), (1,)), ((), ()))
contract_first = (((0,), (0,)), ((), ()))
bf16, f32 = jnp.bfloat16, jnp.float32
MESH = pl.DeviceIdType.MESH
SIDE = 4
ROWS, WIDTH, MODEL, HIDDEN = 768, 256, 2048, 1024
HALF = HIDDEN // 2


def around(k):
    return lax.rem(k + SIDE, SIDE)


class Place:
    def __init__(self):
        fs, tp = lax.axis_index("fs"), lax.axis_index("tp")
        self.z, self.x = fs // SIDE, lax.rem(fs, SIDE)
        self.y, self.core = tp // 2, lax.rem(tp, 2)

    def device(self, z=0, x=0, y=0, core=0):
        fs = around(self.z + z) * SIDE + around(self.x + x)
        tp = around(self.y + y) * 2 + lax.rem(self.core + core, 2)
        return (fs, tp)

    def neighbours(self):
        return [self.device(**{a: d}) for a in ("z", "x", "y") for d in (1, -1)] + [
            self.device(core=1)
        ]


class Ring:
    def __init__(self, place, axis, piece, sems, base):
        self.sems, self.base = sems, base
        at = getattr(place, axis)
        on, back = place.device(**{axis: 1}), place.device(**{axis: -1})
        before, after, across = around(at - 1), around(at + 1), around(at + 2)
        self.sent = [
            (piece(at, 0), on),
            (piece(at, 1), on),
            (piece(at, 1), back),
            (piece(at, 0), back),
            (piece(before, 0), on),
            (piece(after, 1), back),
        ]
        self.landed = [
            piece(before, 0),
            piece(before, 1),
            piece(after, 1),
            piece(after, 0),
            piece(across, 0),
            piece(across, 1),
        ]

    def copy(self, j, ref):
        send, receive = self.sems
        return pltpu.make_async_remote_copy(
            src_ref=ref,
            dst_ref=ref,
            send_sem=send.at[self.base + j],
            recv_sem=receive.at[self.base + j],
            device_id=self.sent[j][1],
            device_id_type=MESH,
        )

    def start(self, *which):
        for j in which:
            self.copy(j, self.sent[j][0]).start()

    def arrive(self, *which):
        for j in which:
            self.copy(j, self.landed[j]).wait_recv()

    def own(self):
        self.start(0, 2, 1, 3)

    def forward(self):
        self.arrive(0)
        self.start(4)
        self.arrive(2)
        self.start(5)

    def near(self):
        self.arrive(1, 3)

    def far(self):
        self.arrive(4, 5)

    def drain(self):
        for j in range(6):
            self.copy(j, self.sent[j][0]).wait_send()


class Partner:
    def __init__(self, place, block, sems, base):
        self.sems, self.base = sems, base
        self.device = place.device(core=1)
        steps = (0, -1, 1, 2)
        self.sent = [block(around(place.y + d), place.core) for d in steps]
        self.landed = [block(around(place.y + d), 1 - place.core) for d in steps]

    def copy(self, j, ref):
        send, receive = self.sems
        return pltpu.make_async_remote_copy(
            src_ref=ref,
            dst_ref=ref,
            send_sem=send.at[self.base + j],
            recv_sem=receive.at[self.base + j],
            device_id=self.device,
            device_id_type=MESH,
        )

    def start(self, *which):
        for j in which:
            self.copy(j, self.sent[j]).start()

    def finish(self):
        for j in range(4):
            self.copy(j, self.landed[j]).wait_recv()

    def drain(self):
        for j in range(4):
            self.copy(j, self.sent[j]).wait_send()


def gather_kernel(
    later_in, earlier_in, cot_in, up_in, down_in, act_out, up_out, down_out,
    act, up, down, load_sem, ring_send, ring_recv, pair_send, pair_recv,
):
    place = Place()
    barrier = pltpu.get_barrier_semaphore()
    for neighbour in place.neighbours():
        pl.semaphore_signal(barrier, inc=1, device_id=neighbour, device_id_type=MESH)

    def act_at(a, y, core, first, count):
        column = pl.multiple_of((y * 2 + core) * WIDTH, WIDTH)
        return act.at[a, pl.ds(first, count), pl.ds(column, WIDTH)]

    def down_at(h, s, first, count):
        return down.at[pl.ds(h * HALF + s * 256, 256), pl.ds(pl.multiple_of(first * 128, 128), count)]

    loads = []
    for a, ref in enumerate((earlier_in, cot_in, later_in)):
        loads.append((ref, act_at(a, place.y, place.core, 0, ROWS)))
    for h in range(2):
        loads.append((up_in.at[:, pl.ds(h * HALF, HALF)], up.at[h, place.z, place.x]))
    loads.append(
        (down_in, down.at[:, pl.ds(pl.multiple_of((place.z * SIDE + place.x) * 128, 128), 128)])
    )
    loads = [pltpu.make_async_copy(s, d, load_sem.at[i]) for i, (s, d) in enumerate(loads)]
    for load in loads:
        load.start()

    sems = (ring_send, ring_recv)
    rings = iter(range(0, 66, 6))
    rows = [
        Ring(place, "y", lambda k, s, a=a: act_at(a, k, place.core, s * 384, 384), sems, next(rings))
        for a in range(3)
    ]
    pairs = [
        Partner(place, lambda y, c, a=a: act_at(a, y, c, 0, ROWS), (pair_send, pair_recv), 4 * a)
        for a in range(3)
    ]
    first, second = [], []
    for h in range(2):
        first.append((
            Ring(place, "z", lambda k, s, h=h: up.at[h, k, place.x, pl.ds(s * 64, 64), :], sems, next(rings)),
            Ring(place, "x", lambda k, s, h=h: down_at(h, s, place.z * SIDE + k, 128), sems, next(rings)),
        ))
        second.append((
            Ring(place, "x", lambda k, s, h=h: up.at[h, :, k, pl.ds(s * 64, 64), :], sems, next(rings)),
            Ring(place, "z", lambda k, s, h=h: down_at(h, s, k * SIDE, 512), sems, next(rings)),
        ))

    def both(stage, name):
        for ring in stage:
            getattr(ring, name)()

    for load in loads:
        load.wait()
    pl.semaphore_wait(barrier, 7)

    both(first[0], "own")
    rows[0].own()
    pairs[0].start(0)
    both(first[0], "forward")
    both(first[1], "own")
    rows[0].forward()
    rows[1].own()
    pairs[1].start(0)
    both(first[0], "near")
    both(first[0], "far")
    both(second[0], "own")
    both(first[1], "forward")
    rows[0].near()
    pairs[0].start(1, 2)
    both(second[0], "forward")
    rows[0].far()
    pairs[0].start(3)
    rows[1].forward()
    rows[2].own()
    pairs[2].start(0)
    rows[1].near()
    pairs[1].start(1, 2)
    both(first[1], "near")
    both(first[1], "far")
    both(second[1], "own")
    both(second[0], "near")
    both(second[0], "far")
    rows[1].far()
    pairs[1].start(3)
    rows[2].forward()
    both(second[1], "forward")
    rows[2].near()
    pairs[2].start(1, 2)
    rows[2].far()
    pairs[2].start(3)
    both(second[1], "near")
    both(second[1], "far")
    for pair in pairs:
        pair.finish()
    stores = [(act.at[a], act_out.at[a]) for a in range(3)]
    stores += [(up.at[h], up_out.at[:, :, :, pl.ds(h * HALF, HALF)]) for h in range(2)]
    stores += [(down, down_out)]
    stores = [pltpu.make_async_copy(s, d, load_sem.at[i]) for i, (s, d) in enumerate(stores)]
    for store in stores:
        store.start()
    for ring in rows + [r for stage in first + second for r in stage]:
        ring.drain()
    for pair in pairs:
        pair.drain()
    for store in stores:
        store.wait()


def gather_all(later_input, earlier_input, cotangent, up_weight, down_weight):
    anywhere = pl.BlockSpec(memory_space=pl.ANY)
    act, up, down = pl.pallas_call(
        gather_kernel,
        out_shape=(
            jax.ShapeDtypeStruct((3, ROWS, MODEL), bf16),
            jax.ShapeDtypeStruct((SIDE, SIDE, 128, HIDDEN), bf16),
            jax.ShapeDtypeStruct((HIDDEN, MODEL), bf16),
        ),
        in_specs=[anywhere] * 5,
        out_specs=(anywhere,) * 3,
        scratch_shapes=[
            pltpu.VMEM((3, ROWS, MODEL), bf16),
            pltpu.VMEM((2, SIDE, SIDE, 128, HALF), bf16),
            pltpu.VMEM((HIDDEN, MODEL), bf16),
            pltpu.SemaphoreType.DMA((6,)),
            pltpu.SemaphoreType.DMA((66,)),
            pltpu.SemaphoreType.DMA((66,)),
            pltpu.SemaphoreType.DMA((12,)),
            pltpu.SemaphoreType.DMA((12,)),
        ],
        compiler_params=pltpu.CompilerParams(
            collective_id=0, has_side_effects=True, vmem_limit_bytes=60 * 2**20
        ),
    )(later_input, earlier_input, cotangent, up_weight, down_weight)
    return act[2], act[0], act[1], up.reshape(MODEL, HIDDEN), down


def side_by_side(arrays, axis, dim, along):
    both = jnp.concatenate(arrays, axis=along)
    filled, at, outs = (lax.psum_scatter(both, axis, scatter_dimension=dim, tiled=True), 0, [])
    for a in arrays:
        outs.append(lax.slice_in_dim(filled, at, at + a.shape[along], axis=along))
        at += a.shape[along]
    return tuple(outs)


def on_device(
    later_input, earlier_input, cotangent, up_weight, down_weight, up_running, down_running
):
    rows = later_input.shape[0]
    factor = float(rows * lax.axis_size("fs")) ** (-0.5)
    columns = up_weight.shape[1]
    later_full, earlier_full, cot_full, up_whole, down_whole = gather_all(
        later_input, earlier_input, cotangent, up_weight, down_weight
    )
    later_up = jnp.dot(later_full, up_whole, preferred_element_type=f32)
    earlier_up = jnp.dot(earlier_full, up_whole, preferred_element_type=f32)
    later_hidden = jnp.square(jax.nn.relu(later_up)).astype(bf16)
    out_part = jnp.dot(later_hidden, down_whole, preferred_element_type=f32)
    hidden_grad = lax.dot_general(cot_full, down_whole, contract_last, preferred_element_type=f32)
    up_grad = (2.0 * jax.nn.relu(earlier_up) * hidden_grad).astype(bf16)
    back_part = lax.dot_general(up_grad, up_whole, contract_last, preferred_element_type=f32)
    later_preact = later_up.astype(bf16)
    earlier_hidden = jnp.square(jax.nn.relu(earlier_up)).astype(bf16)
    out_sum, back_sum = tuple(
        (
            part.astype(f32)
            for part in side_by_side((out_part.astype(bf16), back_part.astype(bf16)), "tp", 1, 0)
        )
    )
    summed = lax.psum_scatter(
        jnp.concatenate(
            (
                lax.dot_general(earlier_full, up_grad, contract_first, preferred_element_type=f32),
                lax.dot_general(cot_full, earlier_hidden, contract_first, preferred_element_type=f32),
            ),
            axis=1,
        ).astype(bf16),
        "fs",
        scatter_dimension=0,
        tiled=True,
    ).astype(f32)
    return (
        out_sum.astype(bf16),
        later_preact,
        back_sum.astype(bf16),
        up_running + summed[:, :columns] * factor,
        down_running + summed[:, columns:] * factor,
    )


def solution(mesh):
    in_specs = (
        P("fs", "tp"),
        P("fs", "tp"),
        P("fs", "tp"),
        P("fs", "tp"),
        P("tp", "fs"),
        P("fs", "tp"),
        P("fs", "tp"),
    )
    out_specs = (P("fs", "tp"),) * 5
    return jax.shard_map(
        on_device, mesh=mesh, in_specs=in_specs, out_specs=out_specs, check_vma=False
    )
```

```python
import jax
import jax.numpy as jnp
from jax import lax
from jax.experimental import pallas as pl
from jax.experimental.pallas import tpu as pltpu
from jax.sharding import PartitionSpec as P

contract_last = (((1,), (1,)), ((), ()))
contract_first = (((0,), (0,)), ((), ()))
bf16, f32 = jnp.bfloat16, jnp.float32
MESH = pl.DeviceIdType.MESH
SIDE = 4
ROWS, WIDTH, MODEL, HIDDEN = 768, 256, 2048, 1024
HALF = HIDDEN // 2
STRIP = ROWS // 2


def around(k):
    return lax.rem(k + SIDE, SIDE)


class Place:
    def __init__(self):
        fs, tp = lax.axis_index("fs"), lax.axis_index("tp")
        self.z, self.x = fs // SIDE, lax.rem(fs, SIDE)
        self.y, self.core = tp // 2, lax.rem(tp, 2)

    def device(self, z=0, x=0, y=0, core=0):
        fs = around(self.z + z) * SIDE + around(self.x + x)
        tp = around(self.y + y) * 2 + lax.rem(self.core + core, 2)
        return (fs, tp)

    def neighbours(self):
        return [self.device(**{a: d}) for a in ("z", "x", "y") for d in (1, -1)] + [
            self.device(core=1)
        ]


class Ring:
    def __init__(self, place, axis, piece, sems, base):
        self.sems, self.base = sems, base
        at = getattr(place, axis)
        on, back = place.device(**{axis: 1}), place.device(**{axis: -1})
        before, after, across = around(at - 1), around(at + 1), around(at + 2)
        self.sent = [
            (piece(at, 0), on),
            (piece(at, 1), on),
            (piece(at, 1), back),
            (piece(at, 0), back),
            (piece(before, 0), on),
            (piece(after, 1), back),
        ]
        self.landed = [
            piece(before, 0),
            piece(before, 1),
            piece(after, 1),
            piece(after, 0),
            piece(across, 0),
            piece(across, 1),
        ]

    def copy(self, j, ref):
        send, receive = self.sems
        return pltpu.make_async_remote_copy(
            src_ref=ref,
            dst_ref=ref,
            send_sem=send.at[self.base + j],
            recv_sem=receive.at[self.base + j],
            device_id=self.sent[j][1],
            device_id_type=MESH,
        )

    def start(self, *which):
        for j in which:
            self.copy(j, self.sent[j][0]).start()

    def arrive(self, *which):
        for j in which:
            self.copy(j, self.landed[j]).wait_recv()

    def own(self):
        self.start(0, 2, 1, 3)

    def forward(self):
        self.arrive(0)
        self.start(4)
        self.arrive(2)
        self.start(5)

    def near(self):
        self.arrive(1, 3)

    def far(self):
        self.arrive(4, 5)

    def drain(self):
        for j in range(6):
            self.copy(j, self.sent[j][0]).wait_send()


class Partner:
    def __init__(self, place, block, sems, base):
        self.sems, self.base = sems, base
        self.device = place.device(core=1)
        steps = (0, -1, 1, 2)
        self.sent = [block(around(place.y + d), place.core) for d in steps]
        self.landed = [block(around(place.y + d), 1 - place.core) for d in steps]

    def copy(self, j, ref):
        send, receive = self.sems
        return pltpu.make_async_remote_copy(
            src_ref=ref,
            dst_ref=ref,
            send_sem=send.at[self.base + j],
            recv_sem=receive.at[self.base + j],
            device_id=self.device,
            device_id_type=MESH,
        )

    def start(self, *which):
        for j in which:
            self.copy(j, self.sent[j]).start()

    def finish(self):
        for j in range(4):
            self.copy(j, self.landed[j]).wait_recv()

    def drain(self):
        for j in range(4):
            self.copy(j, self.sent[j]).wait_send()


class RingSum:
    def __init__(self, place, axis, block, far, near, sems, base):
        self.sems, self.base = sems, base
        at = getattr(place, axis)
        on, back = place.device(**{axis: 1}), place.device(**{axis: -1})
        before, after, across = around(at - 1), around(at + 1), around(at + 2)
        self.mine = [block(at, s) for s in range(2)]
        self.far, self.near = far, near
        self.sent = [
            (block(across, 0), far(0), on),
            (block(across, 1), far(1), back),
            (block(after, 1), near(0, 1), on),
            (block(before, 0), near(1, 0), back),
            (block(after, 0), near(0, 0), on),
            (block(before, 1), near(1, 1), back),
        ]

    def copy(self, j):
        send, receive = self.sems
        src, dst, device = self.sent[j]
        return pltpu.make_async_remote_copy(
            src_ref=src,
            dst_ref=dst,
            send_sem=send.at[self.base + j],
            recv_sem=receive.at[self.base + j],
            device_id=device,
            device_id_type=MESH,
        )

    def begin(self):
        for j in (0, 1, 2, 3):
            self.copy(j).start()

    def middle(self):
        for j in range(2):
            self.copy(j).wait_recv()
            ref = self.sent[4 + j][0]
            ref[...] = (ref[...].astype(f32) + self.far(j)[...].astype(f32)).astype(bf16)
            self.copy(4 + j).start()

    def total(self, s):
        return (
            self.mine[s][...].astype(f32)
            + self.near(0, s)[...].astype(f32)
            + self.near(1, s)[...].astype(f32)
        )

    def arrive(self):
        for j in (2, 3, 4, 5):
            self.copy(j).wait_recv()

    def finish(self):
        self.arrive()
        for s in range(2):
            self.mine[s][...] = self.total(s).astype(bf16)

    def drain(self):
        for j in range(6):
            self.copy(j).wait_send()


def dot(a, b):
    return jnp.dot(a, b, preferred_element_type=f32)


def dot_turned(a, b):
    return lax.dot_general(a, b, contract_last, preferred_element_type=f32)


def layer_kernel(
    factor,
    later_in, earlier_in, cot_in, up_in, down_in, up_run_in, down_run_in,
    out_hbm, pre_hbm, back_hbm, up_run_hbm, down_run_hbm,
    act, turned, up, down, first_up, hidden, grad, pre, part, other, run, up_sum, down_sum,
    far_row, near_row, far_one, near_one, far_two, near_two,
    load_sem, ring_send, ring_recv, pair_send, pair_recv, sum_send, sum_recv,
):
    place = Place()
    barrier = pltpu.get_barrier_semaphore()
    for neighbour in place.neighbours():
        pl.semaphore_signal(barrier, inc=1, device_id=neighbour, device_id_type=MESH)

    def act_at(a, y, core, first, count):
        column = pl.multiple_of((y * 2 + core) * WIDTH, WIDTH)
        return act.at[a, pl.ds(first, count), pl.ds(column, WIDTH)]

    def down_at(h, s, first, count):
        return down.at[pl.ds(h * HALF + s * 256, 256), pl.ds(pl.multiple_of(first * 128, 128), count)]

    loads = []
    for a, ref in enumerate((earlier_in, cot_in, later_in)):
        loads.append((ref, act_at(a, place.y, place.core, 0, ROWS)))
    for h in range(2):
        loads.append((up_in.at[:, pl.ds(h * HALF, HALF)], up.at[h, place.z, place.x]))
    loads.append(
        (down_in, down.at[:, pl.ds(pl.multiple_of((place.z * SIDE + place.x) * 128, 128), 128)])
    )
    loads += [(up_run_in, run.at[0]), (down_run_in, run.at[1])]
    loads = [pltpu.make_async_copy(s, d, load_sem.at[i]) for i, (s, d) in enumerate(loads)]
    for load in loads:
        load.start()

    sems = (ring_send, ring_recv)
    rings = iter(range(0, 66, 6))
    rows = [
        Ring(place, "y", lambda k, s, a=a: act_at(a, k, place.core, s * 384, 384), sems, next(rings))
        for a in range(3)
    ]
    pairs = [
        Partner(place, lambda y, c, a=a: act_at(a, y, c, 0, ROWS), (pair_send, pair_recv), 4 * a)
        for a in range(3)
    ]
    first, second = [], []
    for h in range(2):
        first.append((
            Ring(place, "z", lambda k, s, h=h: up.at[h, k, place.x, pl.ds(s * 64, 64), :], sems, next(rings)),
            Ring(place, "x", lambda k, s, h=h: down_at(h, s, place.z * SIDE + k, 128), sems, next(rings)),
        ))
        second.append((
            Ring(place, "x", lambda k, s, h=h: up.at[h, :, k, pl.ds(s * 64, 64), :], sems, next(rings)),
            Ring(place, "z", lambda k, s, h=h: down_at(h, s, k * SIDE, 512), sems, next(rings)),
        ))

    sems = (sum_send, sum_recv)
    sums = iter(range(0, 60, 6))
    row_sums = [
        RingSum(
            place, "y", lambda k, s, a=a: part.at[a, place.core, k, pl.ds(s * 384, 384), :],
            lambda d, a=a: far_row.at[a, d], lambda d, s, a=a: near_row.at[a, d, s], sems, next(sums),
        )
        for a in range(2)
    ]
    up_one, up_two, down_one, down_two = [], [], [], []
    for h in range(2):
        up_one.append(RingSum(
            place, "x", lambda k, s, h=h: up_sum.at[h, :, k, pl.ds(s * 64, 64), :],
            lambda d, h=h: far_one.at[0, h, d], lambda d, s, h=h: near_one.at[0, h, d, s], sems, next(sums),
        ))
        down_one.append(RingSum(
            place, "z", lambda k, s, h=h: down_sum.at[h, k, :, pl.ds(s * 64, 64), :],
            lambda d, h=h: far_one.at[1, h, d], lambda d, s, h=h: near_one.at[1, h, d, s], sems, next(sums),
        ))
        up_two.append(RingSum(
            place, "z", lambda k, s, h=h: up_sum.at[h, k, place.x, pl.ds(s * 64, 64), :],
            lambda d, h=h: far_two.at[0, h, d], lambda d, s, h=h: near_two.at[0, h, d, s], sems, next(sums),
        ))
        down_two.append(RingSum(
            place, "x", lambda k, s, h=h: down_sum.at[h, place.z, k, pl.ds(s * 64, 64), :],
            lambda d, h=h: far_two.at[1, h, d], lambda d, s, h=h: near_two.at[1, h, d, s], sems, next(sums),
        ))

    def swap(a):
        return pltpu.make_async_remote_copy(
            src_ref=part.at[a, 1 - place.core],
            dst_ref=other.at[a],
            send_sem=pair_send.at[12 + a],
            recv_sem=pair_recv.at[12 + a],
            device_id=place.device(core=1),
            device_id_type=MESH,
        )

    def both(stage, name):
        for ring in stage:
            getattr(ring, name)()

    def strip(m):
        return pl.ds(pl.multiple_of(m * STRIP, STRIP), STRIP)

    def columns(h):
        return pl.ds(h * HALF, HALF)

    def turn(a):
        @pl.loop(0, 8)
        def _(n):
            block = pl.ds(pl.multiple_of(n * 256, 256), 256)
            turned[a, block, :] = act[a, :, block].T

    def up_of(h):
        return up[h].reshape(MODEL, HALF)

    def earlier_up(h):
        @pl.loop(0, 2)
        def _(m):
            value = jnp.maximum(dot(act[0, strip(m), :], up_of(h)), 0.0)
            first_up[strip(m), :] = value
            hidden[strip(m), columns(h)] = jnp.square(value).astype(bf16)

    def hidden_grad(h):
        @pl.loop(0, 2)
        def _(m):
            value = dot_turned(act[1, strip(m), :], down[columns(h), :])
            grad[strip(m), columns(h)] = (2.0 * first_up[strip(m), :] * value).astype(bf16)

    def weight_grad(a, source, target, h):
        @pl.loop(0, 4)
        def _(n):
            block = pl.ds(pl.multiple_of(n * 512, 512), 512)
            value = dot(turned[a, block, :], source[:, columns(h)])
            target[h, n] = value.astype(bf16).reshape(SIDE, 128, HALF)

    def later_up(h):
        @pl.loop(0, 2)
        def _(m):
            value = dot(act[2, strip(m), :], up_of(h))
            pre[strip(m), columns(h)] = value.astype(bf16)
            hidden[strip(m), columns(h)] = jnp.square(jnp.maximum(value, 0.0)).astype(bf16)

    def keep(a, n, m, value):
        value = value.astype(bf16)
        part[a, 0, n, strip(m), :] = value[:, :WIDTH]
        part[a, 1, n, strip(m), :] = value[:, WIDTH:]

    def later_out():
        @pl.loop(0, 4)
        def _(n):
            block = pl.ds(pl.multiple_of(n * 512, 512), 512)

            @pl.loop(0, 2)
            def _(m):
                keep(0, n, m, dot(hidden[strip(m), :], down[:, block]))

    def input_grad():
        @pl.loop(0, 4)
        def _(n):
            @pl.loop(0, 2)
            def _(m):
                weight = jnp.concatenate([up[h, n].reshape(512, HALF) for h in range(2)], axis=1)
                keep(1, n, m, dot_turned(grad[strip(m), :], weight))

    def join(a):
        swap(a).wait_recv()

        @pl.loop(0, 4)
        def _(k):
            part[a, place.core, k] = (
                part[a, place.core, k].astype(f32) + other[a, k].astype(f32)
            ).astype(bf16)

    def add_running(w, ring, h):
        ring.arrive()
        for s in range(2):
            at = run.at[w, pl.ds(s * 64, 64), columns(h)]
            at[...] = at[...] + ring.total(s) * factor

    for load in loads:
        load.wait()
    pl.semaphore_wait(barrier, 7)

    both(first[0], "own")
    rows[0].own()
    pairs[0].start(0)
    both(first[0], "forward")
    both(first[1], "own")
    rows[0].forward()
    rows[1].own()
    pairs[1].start(0)
    both(first[0], "near")
    both(first[0], "far")
    both(second[0], "own")
    both(first[1], "forward")
    rows[0].near()
    pairs[0].start(1, 2)
    both(second[0], "forward")
    rows[0].far()
    pairs[0].start(3)
    pairs[0].finish()
    turn(0)
    rows[1].forward()
    rows[2].own()
    pairs[2].start(0)
    rows[1].near()
    pairs[1].start(1, 2)
    both(first[1], "near")
    both(first[1], "far")
    both(second[1], "own")
    both(second[0], "near")
    both(second[0], "far")
    earlier_up(0)
    rows[1].far()
    pairs[1].start(3)
    rows[2].forward()
    pairs[1].finish()
    turn(1)
    both(second[1], "forward")
    weight_grad(1, hidden, down_sum, 0)
    down_one[0].begin()
    rows[2].near()
    pairs[2].start(1, 2)
    hidden_grad(0)
    weight_grad(0, grad, up_sum, 0)
    up_one[0].begin()
    rows[2].far()
    pairs[2].start(3)
    both(second[1], "near")
    both(second[1], "far")
    earlier_up(1)
    hidden_grad(1)
    weight_grad(1, hidden, down_sum, 1)
    down_one[0].middle()
    up_one[0].middle()
    down_one[1].begin()
    weight_grad(0, grad, up_sum, 1)
    up_one[1].begin()
    input_grad()
    swap(1).start()
    pairs[2].finish()
    later_up(0)
    later_up(1)
    keep_pre = pltpu.make_async_copy(pre, pre_hbm, load_sem.at[0])
    keep_pre.start()
    join(1)
    row_sums[1].begin()
    down_one[0].finish()
    down_two[0].begin()
    up_one[0].finish()
    up_two[0].begin()
    later_out()
    swap(0).start()
    down_one[1].middle()
    up_one[1].middle()
    join(0)
    row_sums[1].middle()
    row_sums[0].begin()
    down_two[0].middle()
    up_two[0].middle()
    down_one[1].finish()
    down_two[1].begin()
    up_one[1].finish()
    up_two[1].begin()
    row_sums[0].middle()
    row_sums[1].finish()
    own = [part.at[a, place.core, place.y] for a in range(2)]
    keep_back = pltpu.make_async_copy(own[1], back_hbm, load_sem.at[1])
    keep_back.start()
    add_running(1, down_two[0], 0)
    add_running(0, up_two[0], 0)
    down_two[1].middle()
    up_two[1].middle()
    row_sums[0].finish()
    keep_out = pltpu.make_async_copy(own[0], out_hbm, load_sem.at[2])
    keep_out.start()
    add_running(1, down_two[1], 1)
    keep_down = pltpu.make_async_copy(run.at[1], down_run_hbm, load_sem.at[3])
    keep_down.start()
    add_running(0, up_two[1], 1)
    keep_up = pltpu.make_async_copy(run.at[0], up_run_hbm, load_sem.at[4])
    keep_up.start()
    for ring in rows + [r for stage in first + second for r in stage]:
        ring.drain()
    for pair in pairs:
        pair.drain()
    for ring in row_sums + up_one + up_two + down_one + down_two:
        ring.drain()
    for a in range(2):
        swap(a).wait_send()
    for store in (keep_pre, keep_back, keep_out, keep_down, keep_up):
        store.wait()


def on_device(*arrays):
    factor = float(ROWS * 16) ** (-0.5)
    anywhere = pl.BlockSpec(memory_space=pl.ANY)
    return pl.pallas_call(
        lambda *refs: layer_kernel(factor, *refs),
        out_shape=(
            jax.ShapeDtypeStruct((ROWS, WIDTH), bf16),
            jax.ShapeDtypeStruct((ROWS, HIDDEN), bf16),
            jax.ShapeDtypeStruct((ROWS, WIDTH), bf16),
            jax.ShapeDtypeStruct((128, HIDDEN), f32),
            jax.ShapeDtypeStruct((128, HIDDEN), f32),
        ),
        in_specs=[anywhere] * 7,
        out_specs=(anywhere,) * 5,
        scratch_shapes=[
            pltpu.VMEM((3, ROWS, MODEL), bf16),
            pltpu.VMEM((2, MODEL, ROWS), bf16),
            pltpu.VMEM((2, SIDE, SIDE, 128, HALF), bf16),
            pltpu.VMEM((HIDDEN, MODEL), bf16),
            pltpu.VMEM((ROWS, HALF), f32),
            pltpu.VMEM((ROWS, HIDDEN), bf16),
            pltpu.VMEM((ROWS, HIDDEN), bf16),
            pltpu.VMEM((ROWS, HIDDEN), bf16),
            pltpu.VMEM((2, 2, SIDE, ROWS, WIDTH), bf16),
            pltpu.VMEM((2, SIDE, ROWS, WIDTH), bf16),
            pltpu.VMEM((2, 128, HIDDEN), f32),
            pltpu.VMEM((2, SIDE, SIDE, 128, HALF), bf16),
            pltpu.VMEM((2, SIDE, SIDE, 128, HALF), bf16),
            pltpu.VMEM((2, 2, STRIP, WIDTH), bf16),
            pltpu.VMEM((2, 2, 2, STRIP, WIDTH), bf16),
            pltpu.VMEM((2, 2, 2, SIDE, 64, HALF), bf16),
            pltpu.VMEM((2, 2, 2, 2, SIDE, 64, HALF), bf16),
            pltpu.VMEM((2, 2, 2, 64, HALF), bf16),
            pltpu.VMEM((2, 2, 2, 2, 64, HALF), bf16),
            pltpu.SemaphoreType.DMA((8,)),
            pltpu.SemaphoreType.DMA((66,)),
            pltpu.SemaphoreType.DMA((66,)),
            pltpu.SemaphoreType.DMA((14,)),
            pltpu.SemaphoreType.DMA((14,)),
            pltpu.SemaphoreType.DMA((60,)),
            pltpu.SemaphoreType.DMA((60,)),
        ],
        compiler_params=pltpu.CompilerParams(
            collective_id=0, has_side_effects=True, vmem_limit_bytes=63 * 2**20
        ),
    )(*arrays)


def solution(mesh):
    in_specs = (
        P("fs", "tp"),
        P("fs", "tp"),
        P("fs", "tp"),
        P("fs", "tp"),
        P("tp", "fs"),
        P("fs", "tp"),
        P("fs", "tp"),
    )
    out_specs = (P("fs", "tp"),) * 5
    return jax.shard_map(
        on_device, mesh=mesh, in_specs=in_specs, out_specs=out_specs, check_vma=False
    )
```

```python
import jax
import jax.numpy as jnp
from jax import lax
from jax.experimental import pallas as pl
from jax.experimental.pallas import tpu as pltpu
from jax.sharding import PartitionSpec as P

contract_last = (((1,), (1,)), ((), ()))
contract_first = (((0,), (0,)), ((), ()))
bf16, f32 = jnp.bfloat16, jnp.float32
MESH = pl.DeviceIdType.MESH
SIDE = 4
ROWS, WIDTH, MODEL, HIDDEN = 768, 256, 2048, 1024
HALF = HIDDEN // 2
STRIP = ROWS // 2
LIMIT = 60 * 2**20


def around(k):
    return lax.rem(k + SIDE, SIDE)


class Place:
    def __init__(self):
        fs, tp = lax.axis_index("fs"), lax.axis_index("tp")
        self.z, self.x = fs // SIDE, lax.rem(fs, SIDE)
        self.y, self.core = tp // 2, lax.rem(tp, 2)

    def device(self, z=0, x=0, y=0, core=0):
        fs = around(self.z + z) * SIDE + around(self.x + x)
        tp = around(self.y + y) * 2 + lax.rem(self.core + core, 2)
        return (fs, tp)

    def neighbours(self):
        return [self.device(**{a: d}) for a in ("z", "x", "y") for d in (1, -1)] + [
            self.device(core=1)
        ]


class Ring:
    def __init__(self, place, axis, piece, two, sems, base):
        self.sems, self.base, self.two = sems, base, two
        at = getattr(place, axis)
        on, back = place.device(**{axis: 1}), place.device(**{axis: -1})
        before, after, across = around(at - 1), around(at + 1), around(at + 2)
        self.sent = [
            (piece(at, 0), on),
            (piece(at, 1), on),
            (piece(at, 1), back),
            (piece(at, 0), back),
            (piece(before, 0), on),
            (piece(after, 1), back),
        ]

    def copy(self, j, ref):
        send, receive = self.sems
        return pltpu.make_async_remote_copy(
            src_ref=ref,
            dst_ref=ref,
            send_sem=send,
            recv_sem=receive.at[self.base + (0, 1, 0, 1, 2, 2)[j]],
            device_id=self.sent[j][1],
            device_id_type=MESH,
        )

    def start(self, *which):
        for j in which:
            self.copy(j, self.sent[j][0]).start()

    def arrive(self, j):
        self.copy(j, self.two).wait_recv()

    def own(self):
        self.start(0, 2, 1, 3)

    def forward(self):
        self.arrive(0)
        self.start(4, 5)

    def near(self):
        self.arrive(1)

    def far(self):
        self.arrive(4)


class Partner:
    def __init__(self, place, block, three, sems, base):
        self.sems, self.base, self.three = sems, base, three
        self.device = place.device(core=1)
        steps = (0, -1, 1, 2)
        self.sent = [block(around(place.y + d), place.core) for d in steps]

    def copy(self, j, ref):
        send, receive = self.sems
        return pltpu.make_async_remote_copy(
            src_ref=ref,
            dst_ref=ref,
            send_sem=send,
            recv_sem=receive.at[self.base + j // 3],
            device_id=self.device,
            device_id_type=MESH,
        )

    def start(self, *which):
        for j in which:
            self.copy(j, self.sent[j]).start()

    def most(self):
        self.copy(0, self.three).wait_recv()

    def last(self):
        self.copy(3, self.sent[3]).wait_recv()


class RingSum:
    def __init__(self, place, axis, block, far, near, sems, base):
        self.sems, self.base, self.both_near = sems, base, near(slice(None), slice(None))
        at = getattr(place, axis)
        on, back = place.device(**{axis: 1}), place.device(**{axis: -1})
        before, after, across = around(at - 1), around(at + 1), around(at + 2)
        self.mine = [block(at, s) for s in range(2)]
        self.far, self.near = far, near
        self.sent = [
            (block(across, 0), far(0), on),
            (block(across, 1), far(1), back),
            (block(after, 1), near(0, 1), on),
            (block(before, 0), near(1, 0), back),
            (block(after, 0), near(0, 0), on),
            (block(before, 1), near(1, 1), back),
        ]

    def copy(self, j):
        send, receive = self.sems
        src, dst, device = self.sent[j]
        return pltpu.make_async_remote_copy(
            src_ref=src,
            dst_ref=dst,
            send_sem=send,
            recv_sem=receive.at[self.base + (0, 1, 2, 2, 2, 2)[j]],
            device_id=device,
            device_id_type=MESH,
        )

    def start(self, *which):
        for j in which:
            self.copy(j).start()

    def begin(self):
        self.start(0, 1, 2, 3)

    def middle(self):
        for j in range(2):
            self.copy(j).wait_recv()
            ref = self.sent[4 + j][0]
            ref[...] = (ref[...].astype(f32) + self.far(j)[...].astype(f32)).astype(bf16)
            self.copy(4 + j).start()

    def total(self, s):
        return (
            self.mine[s][...].astype(f32)
            + self.near(0, s)[...].astype(f32)
            + self.near(1, s)[...].astype(f32)
        )

    def arrive(self):
        send, receive = self.sems
        pltpu.make_async_remote_copy(
            src_ref=self.both_near,
            dst_ref=self.both_near,
            send_sem=send,
            recv_sem=receive.at[self.base + 2],
            device_id=self.sent[0][2],
            device_id_type=MESH,
        ).wait_recv()

    def finish(self, result=None):
        self.arrive()
        for s in range(2):
            target = self.mine[s] if result is None else result.at[pl.ds(s * STRIP, STRIP), :]
            target[...] = self.total(s).astype(bf16)


def dot(a, b):
    return jnp.dot(a, b, preferred_element_type=f32)


def dot_turned(a, b):
    return lax.dot_general(a, b, contract_last, preferred_element_type=f32)


def layer_kernel(
    factor,
    later_in, earlier_in, cot_in, up_in, down_in, up_run_in, down_run_in,
    later_out_ref, pre, back_out, up_run, down_run,
    act, turned, up, down, first_up, hidden, early_hidden, grad, part, other, up_sum, down_sum,
    far_row, near_row, far_one, near_one, far_two, near_two,
    load_sem, send_sem, ring_recv, pair_recv, sum_recv,
):
    place = Place()
    barrier = pltpu.get_barrier_semaphore()
    for neighbour in place.neighbours():
        pl.semaphore_signal(barrier, inc=1, device_id=neighbour, device_id_type=MESH)

    def act_at(a, y, core, first, count):
        column = pl.multiple_of((y * 2 + core) * WIDTH, WIDTH)
        return act.at[a, pl.ds(first, count), pl.ds(column, WIDTH)]

    def down_at(h, s, first, count):
        return down.at[pl.ds(h * HALF + s * 256, 256), pl.ds(pl.multiple_of(first * 128, 128), count)]

    here = place.z * SIDE + place.x
    loads = [(up_in.at[:, pl.ds(h * HALF, HALF)], up.at[h, place.z, place.x]) for h in range(2)]
    loads.insert(1, (down_in, down.at[:, pl.ds(pl.multiple_of(here * 128, 128), 128)]))
    for a, ref in enumerate((earlier_in, cot_in, later_in)):
        loads.insert(2 + 2 * a, (ref, act_at(a, place.y, place.core, 0, ROWS)))
    loads += [(up_run_in, up_run), (down_run_in, down_run)]
    loads = [pltpu.make_async_copy(s, d, load_sem.at[i]) for i, (s, d) in enumerate(loads)]
    for load in loads:
        load.start()

    sems, block = (send_sem.at[0], ring_recv), up.at[0, 0, 0]
    rings = iter(range(0, 69, 3))
    rows = [
        Ring(place, "y", lambda k, s, a=a: act_at(a, k, place.core, s * 384, 384), act.at[a, :, pl.ds(0, WIDTH)],
            (send_sem.at[6], ring_recv), next(rings))
        for a in range(3)
    ]
    pairs = [
        Partner(place, lambda y, c, a=a: act_at(a, y, c, 0, ROWS), act.at[a, :, pl.ds(0, 3 * WIDTH)], (send_sem.at[1], pair_recv), 2 * a)
        for a in range(3)
    ]
    first, second = [], []
    for h in range(2):
        first.append((
            Ring(place, "z", lambda k, s, h=h: up.at[h, k, place.x, pl.ds(s * 64, 64), :], block, sems, next(rings)),
            Ring(place, "x", lambda k, s, h=h: down_at(h, s, place.z * SIDE + k, 128), block, sems, next(rings)),
        ))
        second.append([])
        for d in (0, -1, 1, 2):
            z, x = around(place.z + d), around(place.x + d)
            second[h].append((
                Ring(place, "x", lambda k, s, h=h, z=z: up.at[h, z, k, pl.ds(s * 64, 64), :], block, sems, next(rings)),
                Ring(place, "z", lambda k, s, h=h, x=x: down_at(h, s, k * SIDE + x, 128), block, sems, next(rings)),
            ))

    sums = iter(range(0, 30, 3))
    row_sums = [
        RingSum(
            place, "y", lambda k, s, a=a: part.at[a, place.core, k, pl.ds(s * 384, 384), :],
            lambda d, a=a: far_row.at[a, d], lambda d, s, a=a: near_row.at[a, d, s], (send_sem.at[2], sum_recv), next(sums),
        )
        for a in range(2)
    ]
    up_one, up_two, down_one, down_two = [], [], [], []
    for h in range(2):
        up_one.append(RingSum(
            place, "x", lambda k, s, h=h: up_sum.at[h, :, k, pl.ds(s * 64, 64), :],
            lambda d, h=h: far_one.at[0, h, d], lambda d, s, h=h: near_one.at[0, h, d, s], (send_sem.at[3], sum_recv), next(sums),
        ))
        down_one.append(RingSum(
            place, "z", lambda k, s, h=h: down_sum.at[h, k, :, pl.ds(s * 64, 64), :],
            lambda d, h=h: far_one.at[1, h, d], lambda d, s, h=h: near_one.at[1, h, d, s], (send_sem.at[3], sum_recv), next(sums),
        ))
        up_two.append(RingSum(
            place, "z", lambda k, s, h=h: up_sum.at[h, k, place.x, pl.ds(s * 64, 64), :],
            lambda d, h=h: far_two.at[0, h, d], lambda d, s, h=h: near_two.at[0, h, d, s], (send_sem.at[4], sum_recv), next(sums),
        ))
        down_two.append(RingSum(
            place, "x", lambda k, s, h=h: down_sum.at[h, place.z, k, pl.ds(s * 64, 64), :],
            lambda d, h=h: far_two.at[1, h, d], lambda d, s, h=h: near_two.at[1, h, d, s], (send_sem.at[4], sum_recv), next(sums),
        ))

    order = [around(place.y + d) for d in (2, 1, -1, 0)]

    def swap(a, i):
        return pltpu.make_async_remote_copy(
            src_ref=part.at[a, 1 - place.core, order[i]],
            dst_ref=other.at[a, order[i]],
            send_sem=send_sem.at[5],
            recv_sem=pair_recv.at[6 + 4 * a + i],
            device_id=place.device(core=1),
            device_id_type=MESH,
        )

    def sent(i, ref):
        pltpu.make_async_remote_copy(
            src_ref=ref,
            dst_ref=ref,
            send_sem=send_sem.at[i],
            recv_sem=pair_recv.at[0],
            device_id=place.device(core=1),
            device_id_type=MESH,
        ).wait_send()

    def both(stage, name):
        for ring in stage:
            getattr(ring, name)()

    def strip(m):
        return pl.ds(pl.multiple_of(m * STRIP, STRIP), STRIP)

    def columns(h):
        return pl.ds(h * HALF, HALF)

    def turn(a, core, start, stop):
        @pl.loop(start, stop)
        def _(d):
            block = pl.ds(pl.multiple_of((around(place.y + d) * 2 + core) * WIDTH, WIDTH), WIDTH)
            turned[a, block, :] = act[a, :, block].T

    def up_of(h):
        return up[h].reshape(MODEL, HALF)

    def earlier_up(h):
        @pl.loop(0, 2)
        def _(m):
            value = jnp.maximum(dot(act[0, strip(m), :], up_of(h)), 0.0)
            first_up[strip(m), :] = value
            early_hidden[strip(m), columns(h)] = jnp.square(value).astype(bf16)

    def hidden_grad(h):
        @pl.loop(0, 2)
        def _(m):
            value = dot_turned(act[1, strip(m), :], down[columns(h), :])
            grad[strip(m), columns(h)] = (2.0 * first_up[strip(m), :] * value).astype(bf16)

    def weight_grad(a, source, target, h):
        @pl.loop(0, 4)
        def _(n):
            block = pl.ds(pl.multiple_of(n * 512, 512), 512)
            value = dot(turned[a, block, :], source[:, columns(h)])
            target[h, n] = value.astype(bf16).reshape(SIDE, 128, HALF)

    def later_up(h):
        @pl.loop(0, 2)
        def _(m):
            value = dot(act[2, strip(m), :], up_of(h))
            pre[strip(m), columns(h)] = value.astype(bf16)
            hidden[strip(m), columns(h)] = jnp.square(jnp.maximum(value, 0.0)).astype(bf16)

    def keep(a, n, m, value):
        value = value.astype(bf16)
        part[a, 0, n, strip(m), :] = value[:, :WIDTH]
        part[a, 1, n, strip(m), :] = value[:, WIDTH:]

    def later_out(i):
        n = order[i]
        block = pl.ds(pl.multiple_of(n * 512, 512), 512)

        @pl.loop(0, 2)
        def _(m):
            keep(0, n, m, dot(hidden[strip(m), :], down[:, block]))

        swap(0, i).start()

    def input_grad(i):
        n = order[i]

        @pl.loop(0, 2)
        def _(m):
            weight = jnp.concatenate([up[h, n].reshape(512, HALF) for h in range(2)], axis=1)
            keep(1, n, m, dot_turned(grad[strip(m), :], weight))

        swap(1, i).start()

    def join(a, i):
        swap(a, i).wait_recv()
        n = order[i]
        part[a, place.core, n] = (
            part[a, place.core, n].astype(f32) + other[a, n].astype(f32)
        ).astype(bf16)
        row_sums[a].start(*((0, 1), (2,), (3,), ())[i])

    def add_running(w, ring, h):
        ring.arrive()
        for s in range(2):
            at = (up_run, down_run)[w].at[pl.ds(s * 64, 64), columns(h)]
            at[...] = at[...] + ring.total(s) * factor

    pl.semaphore_wait(barrier, 7)
    loads[0].wait()
    loads[1].wait()

    both(first[0], "own")
    both(second[0][0], "own")
    loads[2].wait()
    rows[0].own()
    pairs[0].start(0)
    for load in loads[3:]:
        load.wait()
    both(first[0], "forward")
    both(first[0], "near")
    both(second[0][1], "own")
    both(second[0][2], "own")
    both(second[0][0], "forward")
    rows[0].forward()
    rows[1].own()
    pairs[1].start(0)
    both(first[0], "far")
    both(second[0][3], "own")
    both(second[0][1], "forward")
    rows[0].near()
    pairs[0].start(1, 2)
    both(second[0][2], "forward")
    rows[0].far()
    pairs[0].start(3)
    both(second[0][3], "forward")
    both(first[1], "own")
    both(second[1][0], "own")
    pairs[0].most()
    pairs[0].last()
    rows[1].forward()
    rows[2].own()
    pairs[2].start(0)
    turn(0, place.core, -1, 3)
    turn(0, 1 - place.core, -1, 3)
    rows[1].near()
    pairs[1].start(1, 2)
    for ring in second[0]:
        both(ring, "near")
        both(ring, "far")
    both(first[1], "forward")
    both(first[1], "near")
    both(second[1][1], "own")
    both(second[1][2], "own")
    earlier_up(0)
    rows[1].far()
    pairs[1].start(3)
    both(second[1][0], "forward")
    turn(1, place.core, -1, 3)
    pairs[1].most()
    turn(1, 1 - place.core, -1, 2)
    both(first[1], "far")
    both(second[1][3], "own")
    pairs[1].last()
    turn(1, 1 - place.core, 2, 3)
    hidden_grad(0)
    rows[2].forward()
    both(second[1][1], "forward")
    weight_grad(1, early_hidden, down_sum, 0)
    both(second[1][2], "forward")
    rows[2].near()
    pairs[2].start(1, 2)
    weight_grad(0, grad, up_sum, 0)
    both(second[1][3], "forward")
    down_one[0].begin()
    up_one[0].begin()
    rows[2].far()
    pairs[2].start(3)
    pairs[2].most()
    pairs[2].last()
    later_up(0)
    for ring in second[1]:
        both(ring, "near")
        both(ring, "far")
    earlier_up(1)
    hidden_grad(1)
    input_grad(0)
    input_grad(1)
    input_grad(2)
    join(1, 0)
    down_one[0].middle()
    up_one[0].middle()
    input_grad(3)
    join(1, 1)
    weight_grad(1, early_hidden, down_sum, 1)
    down_one[1].begin()
    join(1, 2)
    weight_grad(0, grad, up_sum, 1)
    up_one[1].begin()
    join(1, 3)
    later_up(1)
    row_sums[1].middle()
    later_out(0)
    later_out(1)
    down_one[0].finish()
    up_one[0].finish()
    later_out(2)
    join(0, 0)
    later_out(3)
    join(0, 1)
    down_one[1].middle()
    up_one[1].middle()
    down_two[0].begin()
    up_two[0].begin()
    join(0, 2)
    join(0, 3)
    row_sums[1].finish(back_out)
    row_sums[0].middle()
    down_one[1].finish()
    down_two[1].begin()
    up_one[1].finish()
    up_two[1].begin()
    down_two[0].middle()
    up_two[0].middle()
    row_sums[0].finish(later_out_ref)
    down_two[1].middle()
    up_two[1].middle()
    add_running(1, down_two[0], 0)
    add_running(0, up_two[0], 0)
    add_running(1, down_two[1], 1)
    add_running(0, up_two[1], 1)
    sent(0, act.at[:, pl.ds(0, 640), :])
    sent(1, act.at[:, pl.ds(0, 384), :])
    sent(2, act.at[0, pl.ds(0, 576), :])
    sent(3, act.at[pl.ds(0, 2)])
    sent(4, act.at[0, pl.ds(0, 384), :])
    sent(5, act.at[0])
    sent(6, act.at[pl.ds(0, 2), pl.ds(0, 432), :])


def store_kernel(*refs):
    sources, results, sem = refs[:5], refs[5:10], refs[10]
    copies = [
        pltpu.make_async_copy(src, dst, sem.at[i]) for i, (src, dst) in enumerate(zip(sources, results))
    ]
    for copy in copies:
        copy.start()
    for copy in copies:
        copy.wait()


def on_device(*arrays):
    factor = float(ROWS * 16) ** (-0.5)
    anywhere = pl.BlockSpec(memory_space=pl.ANY)
    inside = pl.BlockSpec(memory_space=pltpu.VMEM)
    kept = [
        ((ROWS, WIDTH), bf16),
        ((ROWS, HIDDEN), bf16),
        ((ROWS, WIDTH), bf16),
        ((128, HIDDEN), f32),
        ((128, HIDDEN), f32),
    ]
    results = pl.pallas_call(
        lambda *refs: layer_kernel(factor, *refs),
        out_shape=tuple(pltpu.VMEM(shape, kind) for shape, kind in kept),
        in_specs=[anywhere] * 7,
        out_specs=(inside,) * 5,
        scratch_shapes=[
            pltpu.VMEM((3, ROWS, MODEL), bf16),
            pltpu.VMEM((2, MODEL, ROWS), bf16),
            pltpu.VMEM((2, SIDE, SIDE, 128, HALF), bf16),
            pltpu.VMEM((HIDDEN, MODEL), bf16),
            pltpu.VMEM((ROWS, HALF), f32),
            pltpu.VMEM((ROWS, HIDDEN), bf16),
            pltpu.VMEM((ROWS, HIDDEN), bf16),
            pltpu.VMEM((ROWS, HIDDEN), bf16),
            pltpu.VMEM((2, 2, SIDE, ROWS, WIDTH), bf16),
            pltpu.VMEM((2, SIDE, ROWS, WIDTH), bf16),
            pltpu.VMEM((2, SIDE, SIDE, 128, HALF), bf16),
            pltpu.VMEM((2, SIDE, SIDE, 128, HALF), bf16),
            pltpu.VMEM((2, 2, STRIP, WIDTH), bf16),
            pltpu.VMEM((2, 2, 2, STRIP, WIDTH), bf16),
            pltpu.VMEM((2, 2, 2, SIDE, 64, HALF), bf16),
            pltpu.VMEM((2, 2, 2, 2, SIDE, 64, HALF), bf16),
            pltpu.VMEM((2, 2, 2, 64, HALF), bf16),
            pltpu.VMEM((2, 2, 2, 2, 64, HALF), bf16),
            pltpu.SemaphoreType.DMA((8,)),
            pltpu.SemaphoreType.DMA((7,)),
            pltpu.SemaphoreType.DMA((69,)),
            pltpu.SemaphoreType.DMA((14,)),
            pltpu.SemaphoreType.DMA((30,)),
        ],
        compiler_params=pltpu.CompilerParams(
            collective_id=0, has_side_effects=True, vmem_limit_bytes=LIMIT
        ),
    )(*arrays)
    return pl.pallas_call(
        store_kernel,
        out_shape=tuple(jax.ShapeDtypeStruct(shape, kind) for shape, kind in kept),
        in_specs=[inside] * 5,
        out_specs=(anywhere,) * 5,
        scratch_shapes=[pltpu.SemaphoreType.DMA((5,))],
        compiler_params=pltpu.CompilerParams(vmem_limit_bytes=2**20),
    )(*[pltpu.with_memory_space_constraint(r, pltpu.VMEM) for r in results])


def solution(mesh):
    in_specs = (
        P("fs", "tp"),
        P("fs", "tp"),
        P("fs", "tp"),
        P("fs", "tp"),
        P("tp", "fs"),
        P("fs", "tp"),
        P("fs", "tp"),
    )
    out_specs = (P("fs", "tp"),) * 5
    return jax.shard_map(
        on_device, mesh=mesh, in_specs=in_specs, out_specs=out_specs, check_vma=False
    )
```

```python
import jax
import jax.numpy as jnp
from jax import lax
from jax.experimental import pallas as pl
from jax.experimental.pallas import tpu as pltpu
from jax.sharding import PartitionSpec as P

contract_last = (((1,), (1,)), ((), ()))
contract_first = (((0,), (0,)), ((), ()))
bf16, f32 = jnp.bfloat16, jnp.float32
MESH = pl.DeviceIdType.MESH
SIDE = 4
ROWS, WIDTH, MODEL, HIDDEN = 768, 256, 2048, 1024
HALF = HIDDEN // 2
STRIP = ROWS // 2
LIMIT = 60 * 2**20


def around(k):
    return lax.rem(k + SIDE, SIDE)


class Place:
    def __init__(self):
        fs, tp = lax.axis_index("fs"), lax.axis_index("tp")
        self.z, self.x = fs // SIDE, lax.rem(fs, SIDE)
        self.y, self.core = tp // 2, lax.rem(tp, 2)

    def device(self, z=0, x=0, y=0, core=0):
        fs = around(self.z + z) * SIDE + around(self.x + x)
        tp = around(self.y + y) * 2 + lax.rem(self.core + core, 2)
        return (fs, tp)

    def neighbours(self):
        return [self.device(**{a: d}) for a in ("z", "x", "y") for d in (1, -1)] + [
            self.device(core=1)
        ]


class Ring:
    def __init__(self, place, axis, piece, two, sems, bases, four=None):
        self.sems, self.two, self.four = sems, two, four
        self.last = 2 if four is None else 1
        self.base = bases[0]
        del bases[: self.last + 1]
        at = getattr(place, axis)
        on, back = place.device(**{axis: 1}), place.device(**{axis: -1})
        before, after, across = around(at - 1), around(at + 1), around(at + 2)
        self.sent = [
            (piece(at, 0), on),
            (piece(at, 1), on),
            (piece(at, 1), back),
            (piece(at, 0), back),
            (piece(before, 0), on),
            (piece(after, 1), back),
        ]

    def copy(self, j, ref):
        send, receive = self.sems
        return pltpu.make_async_remote_copy(
            src_ref=ref,
            dst_ref=ref,
            send_sem=send,
            recv_sem=receive.at[self.base + (0, 1, 0, 1, self.last, self.last)[j]],
            device_id=self.sent[j][1],
            device_id_type=MESH,
        )

    def start(self, *which):
        for j in which:
            self.copy(j, self.sent[j][0]).start()

    def arrive(self, j):
        self.copy(j, self.two).wait_recv()

    def own(self):
        self.start(0, 2, 1, 3)

    def forward(self):
        self.arrive(0)
        self.start(4, 5)

    def near(self):
        self.arrive(1)

    def far(self):
        self.arrive(4)

    def rest(self):
        self.copy(1, self.four).wait_recv()


class Partner:
    def __init__(self, place, block, three, sems, base):
        self.sems, self.base, self.three = sems, base, three
        self.device = place.device(core=1)
        steps = (0, -1, 1, 2)
        self.sent = [block(around(place.y + d), place.core) for d in steps]

    def copy(self, j, ref):
        send, receive = self.sems
        return pltpu.make_async_remote_copy(
            src_ref=ref,
            dst_ref=ref,
            send_sem=send,
            recv_sem=receive.at[self.base + j // 3],
            device_id=self.device,
            device_id_type=MESH,
        )

    def start(self, *which):
        for j in which:
            self.copy(j, self.sent[j]).start()

    def most(self):
        self.copy(0, self.three).wait_recv()

    def last(self):
        self.copy(3, self.sent[3]).wait_recv()


class RingSum:
    def __init__(self, place, axis, block, far, near, sems, base):
        self.sems, self.base = sems, base
        self.both_far, self.both_near = far(slice(None)), near(slice(None), slice(None))
        at = getattr(place, axis)
        on, back = place.device(**{axis: 1}), place.device(**{axis: -1})
        before, after, across = around(at - 1), around(at + 1), around(at + 2)
        self.mine = [block(at, s) for s in range(2)]
        self.far, self.near = far, near
        self.sent = [
            (block(across, 0), far(0), on),
            (block(across, 1), far(1), back),
            (block(after, 1), near(0, 1), on),
            (block(before, 0), near(1, 0), back),
            (block(after, 0), near(0, 0), on),
            (block(before, 1), near(1, 1), back),
        ]

    def copy(self, j):
        send, receive = self.sems
        src, dst, device = self.sent[j]
        return pltpu.make_async_remote_copy(
            src_ref=src,
            dst_ref=dst,
            send_sem=send,
            recv_sem=receive.at[self.base + (0, 0, 1, 1, 1, 1)[j]],
            device_id=device,
            device_id_type=MESH,
        )

    def start(self, *which):
        for j in which:
            self.copy(j).start()

    def begin(self):
        self.start(0, 1, 2, 3)

    def receive(self, ref, k):
        send, receive = self.sems
        pltpu.make_async_remote_copy(
            src_ref=ref,
            dst_ref=ref,
            send_sem=send,
            recv_sem=receive.at[self.base + k],
            device_id=self.sent[0][2],
            device_id_type=MESH,
        ).wait_recv()

    def middle(self):
        self.receive(self.both_far, 0)
        for j in range(2):
            ref = self.sent[4 + j][0]
            ref[...] = (ref[...].astype(f32) + self.far(j)[...].astype(f32)).astype(bf16)
        self.start(4, 5)

    def total(self, s):
        return (
            self.mine[s][...].astype(f32)
            + self.near(0, s)[...].astype(f32)
            + self.near(1, s)[...].astype(f32)
        )

    def arrive(self):
        self.receive(self.both_near, 1)

    def finish(self, result=None):
        self.arrive()
        for s in range(2):
            target = self.mine[s] if result is None else result.at[pl.ds(s * STRIP, STRIP), :]
            target[...] = self.total(s).astype(bf16)


def dot(a, b):
    return jnp.dot(a, b, preferred_element_type=f32)


def dot_turned(a, b):
    return lax.dot_general(a, b, contract_last, preferred_element_type=f32)


def layer_kernel(
    factor,
    later_in, earlier_in, cot_in, up_in, down_in, up_run_in, down_run_in,
    later_out_ref, pre, back_out, up_run, down_run,
    act, turned, up, down, first_up, hidden, early_hidden, grad, part, other, up_sum, down_sum,
    far_row, near_row, far_one, near_one, far_two, near_two,
    load_sem, send_sem, ring_recv, pair_recv, sum_recv,
):
    place = Place()
    barrier = pltpu.get_barrier_semaphore()
    for neighbour in place.neighbours():
        pl.semaphore_signal(barrier, inc=1, device_id=neighbour, device_id_type=MESH)

    def act_at(a, y, core, first, count):
        column = pl.multiple_of((y * 2 + core) * WIDTH, WIDTH)
        return act.at[a, pl.ds(first, count), pl.ds(column, WIDTH)]

    def down_at(h, s, first, count):
        return down.at[pl.ds(h * HALF + s * 256, 256), pl.ds(pl.multiple_of(first * 128, 128), count)]

    here = place.z * SIDE + place.x
    loads = [(up_in.at[:, pl.ds(h * HALF, HALF)], up.at[h, place.z, place.x]) for h in range(2)]
    loads.insert(1, (down_in, down.at[:, pl.ds(pl.multiple_of(here * 128, 128), 128)]))
    for a, ref in enumerate((earlier_in, cot_in, later_in)):
        loads.insert(2 + 2 * a, (ref, act_at(a, place.y, place.core, 0, ROWS)))
    loads += [(up_run_in, up_run), (down_run_in, down_run)]
    loads = [pltpu.make_async_copy(s, d, load_sem.at[i]) for i, (s, d) in enumerate(loads)]
    for load in loads:
        load.start()

    sems, block, pair = (send_sem.at[0], ring_recv), up.at[0, 0, 0], up.at[0, 0, pl.ds(0, 2)]
    rings = list(range(41))
    rows = [
        Ring(place, "y", lambda k, s, a=a: act_at(a, k, place.core, s * 384, 384), act.at[a, :, pl.ds(0, WIDTH)],
            (send_sem.at[6], ring_recv), rings)
        for a in range(3)
    ]
    pairs = [
        Partner(place, lambda y, c, a=a: act_at(a, y, c, 0, ROWS), act.at[a, :, pl.ds(0, 3 * WIDTH)], (send_sem.at[1], pair_recv), 2 * a)
        for a in range(3)
    ]
    first, second = [], []
    for h in range(2):
        first.append((
            Ring(place, "z", lambda k, s, h=h: up.at[h, k, place.x, pl.ds(s * 64, 64), :], block, sems, rings),
            Ring(place, "x", lambda k, s, h=h: down_at(h, s, place.z * SIDE + k, 128), block, sems, rings),
        ))
    for d in (0, -1, 1, 2):
        z, x = around(place.z + d), around(place.x + d)
        second.append((
            Ring(place, "x", lambda k, s, z=z: up.at[0, z, k, pl.ds(s * 64, 64), :], block, sems, rings, pair),
            Ring(place, "z", lambda k, s, x=x: down_at(0, s, k * SIDE + x, 128), block, sems, rings, pair),
        ))
    last = (
        Ring(place, "x", lambda k, s: up.at[1, :, k, pl.ds(s * 64, 64), :], up.at[0, 0], sems, rings, up.at[0, pl.ds(0, 2)]),
        Ring(place, "z", lambda k, s: down_at(1, s, k * SIDE, 512), up.at[0, 0], sems, rings, up.at[0, pl.ds(0, 2)]),
    )

    sums = iter(range(0, 32, 2))
    row_sums = [
        RingSum(
            place, "y", lambda k, s, a=a: part.at[a, place.core, k, pl.ds(s * 384, 384), :],
            lambda d, a=a: far_row.at[a, d], lambda d, s, a=a: near_row.at[a, d, s], (send_sem.at[2], sum_recv), next(sums),
        )
        for a in range(2)
    ]
    one, two = (send_sem.at[3], sum_recv), (send_sem.at[4], sum_recv)
    first_sums = (
        RingSum(
            place, "z", lambda k, s: down_sum.at[0, k, :, pl.ds(s * 64, 64), :],
            lambda d: far_one.at[1, 0, d], lambda d, s: near_one.at[1, 0, d, s], one, next(sums),
        ),
        RingSum(
            place, "x", lambda k, s: up_sum.at[0, :, k, pl.ds(s * 64, 64), :],
            lambda d: far_one.at[0, 0, d], lambda d, s: near_one.at[0, 0, d, s], one, next(sums),
        ),
    )
    down_lines, up_lines, second_sums = [], [], []
    for q in (2, 1, -1, 0):
        z, x = around(place.z + q), around(place.x + q)
        down_lines.append(RingSum(
            place, "z", lambda k, s, x=x: down_sum.at[1, k, x, pl.ds(s * 64, 64), :],
            lambda d, x=x: far_one.at[1, 1, d, x], lambda d, s, x=x: near_one.at[1, 1, d, s, x], one, next(sums),
        ))
        up_lines.append(RingSum(
            place, "x", lambda k, s, z=z: up_sum.at[1, z, k, pl.ds(s * 64, 64), :],
            lambda d, z=z: far_one.at[0, 1, d, z], lambda d, s, z=z: near_one.at[0, 1, d, s, z], one, next(sums),
        ))
    lines = list(zip(down_lines, up_lines))
    for h in range(2):
        second_sums.append((
            RingSum(
                place, "x", lambda k, s, h=h: down_sum.at[h, place.z, k, pl.ds(s * 64, 64), :],
                lambda d, h=h: far_two.at[1, h, d], lambda d, s, h=h: near_two.at[1, h, d, s], two, next(sums),
            ),
            RingSum(
                place, "z", lambda k, s, h=h: up_sum.at[h, k, place.x, pl.ds(s * 64, 64), :],
                lambda d, h=h: far_two.at[0, h, d], lambda d, s, h=h: near_two.at[0, h, d, s], two, next(sums),
            ),
        ))

    order = [around(place.y + d) for d in (2, 1, -1, 0)]

    def swap(a, i):
        return pltpu.make_async_remote_copy(
            src_ref=part.at[a, 1 - place.core, order[i]],
            dst_ref=other.at[a, order[i]],
            send_sem=send_sem.at[5],
            recv_sem=pair_recv.at[6 + 4 * a + i],
            device_id=place.device(core=1),
            device_id_type=MESH,
        )

    def sent(i, ref):
        pltpu.make_async_remote_copy(
            src_ref=ref,
            dst_ref=ref,
            send_sem=send_sem.at[i],
            recv_sem=pair_recv.at[0],
            device_id=place.device(core=1),
            device_id_type=MESH,
        ).wait_send()

    def both(stage, name):
        for ring in stage:
            getattr(ring, name)()

    def strip(m):
        return pl.ds(pl.multiple_of(m * STRIP, STRIP), STRIP)

    def columns(h):
        return pl.ds(h * HALF, HALF)

    def turn(a, core, start, stop):
        @pl.loop(start, stop)
        def _(d):
            block = pl.ds(pl.multiple_of((around(place.y + d) * 2 + core) * WIDTH, WIDTH), WIDTH)
            turned[a, block, :] = act[a, :, block].T

    def up_of(h):
        return up[h].reshape(MODEL, HALF)

    def earlier_up(h):
        @pl.loop(0, 2)
        def _(m):
            value = jnp.maximum(dot(act[0, strip(m), :], up_of(h)), 0.0)
            first_up[strip(m), :] = value
            early_hidden[strip(m), columns(h)] = jnp.square(value).astype(bf16)

    def hidden_grad(h):
        @pl.loop(0, 2)
        def _(m):
            value = dot_turned(act[1, strip(m), :], down[columns(h), :])
            grad[strip(m), columns(h)] = (2.0 * first_up[strip(m), :] * value).astype(bf16)

    def weight_grad(a, source, target, h):
        @pl.loop(0, 4)
        def _(n):
            block = pl.ds(pl.multiple_of(n * 512, 512), 512)
            value = dot(turned[a, block, :], source[:, columns(h)])
            target[h, n] = value.astype(bf16).reshape(SIDE, 128, HALF)

    def later_up(h):
        @pl.loop(0, 2)
        def _(m):
            value = dot(act[2, strip(m), :], up_of(h))
            pre[strip(m), columns(h)] = value.astype(bf16)
            hidden[strip(m), columns(h)] = jnp.square(jnp.maximum(value, 0.0)).astype(bf16)

    def keep(a, n, m, value):
        value = value.astype(bf16)
        part[a, 0, n, strip(m), :] = value[:, :WIDTH]
        part[a, 1, n, strip(m), :] = value[:, WIDTH:]

    def later_out(i):
        n = order[i]
        block = pl.ds(pl.multiple_of(n * 512, 512), 512)

        @pl.loop(0, 2)
        def _(m):
            keep(0, n, m, dot(hidden[strip(m), :], down[:, block]))

        swap(0, i).start()

    def input_grad(i):
        n = order[i]

        @pl.loop(0, 2)
        def _(m):
            weight = jnp.concatenate([up[h, n].reshape(512, HALF) for h in range(2)], axis=1)
            keep(1, n, m, dot_turned(grad[strip(m), :], weight))

        swap(1, i).start()

    def join(a, i):
        swap(a, i).wait_recv()
        n = order[i]
        part[a, place.core, n] = (
            part[a, place.core, n].astype(f32) + other[a, n].astype(f32)
        ).astype(bf16)
        row_sums[a].start(*((0, 1), (2,), (3,), ())[i])

    def add_running(w, ring, h):
        ring.arrive()
        for s in range(2):
            at = (up_run, down_run)[w].at[pl.ds(s * 64, 64), columns(h)]
            at[...] = at[...] + ring.total(s) * factor

    pl.semaphore_wait(barrier, 7)
    loads[0].wait()
    loads[1].wait()

    both(first[0], "own")
    both(second[0], "own")
    loads[2].wait()
    rows[0].own()
    pairs[0].start(0)
    for load in loads[3:]:
        load.wait()
    both(first[0], "forward")
    both(first[1], "own")
    both(first[0], "near")
    both(second[1], "own")
    both(second[2], "own")
    both(second[0], "forward")
    rows[0].forward()
    rows[1].own()
    pairs[1].start(0)
    both(first[0], "far")
    both(second[3], "own")
    both(first[1], "forward")
    both(second[1], "forward")
    rows[0].near()
    pairs[0].start(1, 2)
    rows[0].far()
    pairs[0].start(3)
    both(second[2], "forward")
    both(second[3], "forward")
    rows[1].forward()
    rows[2].own()
    pairs[2].start(0)
    both(first[1], "near")
    both(first[1], "far")
    both(last, "own")
    pairs[0].most()
    pairs[0].last()
    turn(0, place.core, -1, 3)
    turn(0, 1 - place.core, -1, 3)
    rows[1].near()
    pairs[1].start(1, 2)
    for ring in second:
        both(ring, "rest")
    earlier_up(0)
    rows[1].far()
    pairs[1].start(3)
    turn(1, place.core, -1, 3)
    pairs[1].most()
    turn(1, 1 - place.core, -1, 2)
    pairs[1].last()
    turn(1, 1 - place.core, 2, 3)
    rows[2].forward()
    both(last, "forward")
    weight_grad(1, early_hidden, down_sum, 0)
    first_sums[0].begin()
    hidden_grad(0)
    rows[2].near()
    pairs[2].start(1, 2)
    weight_grad(0, grad, up_sum, 0)
    first_sums[1].begin()
    rows[2].far()
    pairs[2].start(3)
    pairs[2].most()
    pairs[2].last()
    later_up(0)
    both(last, "rest")
    earlier_up(1)
    hidden_grad(1)
    input_grad(0)
    input_grad(1)
    both(first_sums, "middle")
    weight_grad(1, early_hidden, down_sum, 1)
    both(down_lines[:3], "begin")
    join(1, 0)
    weight_grad(0, grad, up_sum, 1)
    both(up_lines[:3], "begin")
    join(1, 1)
    input_grad(2)
    input_grad(3)
    later_up(1)
    join(1, 2)
    join(1, 3)
    both(first_sums, "finish")
    both(second_sums[0], "begin")
    row_sums[1].middle()
    later_out(0)
    later_out(1)
    for line in lines[:3]:
        both(line, "middle")
    both(lines[3], "begin")
    later_out(2)
    join(0, 0)
    later_out(3)
    join(0, 1)
    both(second_sums[0], "middle")
    join(0, 2)
    join(0, 3)
    row_sums[1].finish(back_out)
    row_sums[0].middle()
    both(lines[0], "finish")
    for ring in second_sums[1]:
        ring.start(0, 1)
    both(lines[1], "finish")
    both(lines[2], "finish")
    for ring in second_sums[1]:
        ring.start(2, 3)
    both(lines[3], "middle")
    both(second_sums[1], "middle")
    add_running(1, second_sums[0][0], 0)
    add_running(0, second_sums[0][1], 0)
    row_sums[0].finish(later_out_ref)
    both(lines[3], "finish")
    add_running(1, second_sums[1][0], 1)
    add_running(0, second_sums[1][1], 1)
    sent(0, act.at[:, pl.ds(0, 640), :])
    sent(1, act.at[:, pl.ds(0, 384), :])
    sent(2, act.at[0, pl.ds(0, 576), :])
    sent(3, act.at[pl.ds(0, 2)])
    sent(4, act.at[0, pl.ds(0, 384), :])
    sent(5, act.at[0])
    sent(6, act.at[pl.ds(0, 2), pl.ds(0, 432), :])


def store_kernel(*refs):
    sources, results, sem = refs[:5], refs[5:10], refs[10]
    copies = [
        pltpu.make_async_copy(src, dst, sem.at[i]) for i, (src, dst) in enumerate(zip(sources, results))
    ]
    for copy in copies:
        copy.start()
    for copy in copies:
        copy.wait()


def on_device(*arrays):
    factor = float(ROWS * 16) ** (-0.5)
    anywhere = pl.BlockSpec(memory_space=pl.ANY)
    inside = pl.BlockSpec(memory_space=pltpu.VMEM)
    kept = [
        ((ROWS, WIDTH), bf16),
        ((ROWS, HIDDEN), bf16),
        ((ROWS, WIDTH), bf16),
        ((128, HIDDEN), f32),
        ((128, HIDDEN), f32),
    ]
    results = pl.pallas_call(
        lambda *refs: layer_kernel(factor, *refs),
        out_shape=tuple(pltpu.VMEM(shape, kind) for shape, kind in kept),
        in_specs=[anywhere] * 7,
        out_specs=(inside,) * 5,
        scratch_shapes=[
            pltpu.VMEM((3, ROWS, MODEL), bf16),
            pltpu.VMEM((2, MODEL, ROWS), bf16),
            pltpu.VMEM((2, SIDE, SIDE, 128, HALF), bf16),
            pltpu.VMEM((HIDDEN, MODEL), bf16),
            pltpu.VMEM((ROWS, HALF), f32),
            pltpu.VMEM((ROWS, HIDDEN), bf16),
            pltpu.VMEM((ROWS, HIDDEN), bf16),
            pltpu.VMEM((ROWS, HIDDEN), bf16),
            pltpu.VMEM((2, 2, SIDE, ROWS, WIDTH), bf16),
            pltpu.VMEM((2, SIDE, ROWS, WIDTH), bf16),
            pltpu.VMEM((2, SIDE, SIDE, 128, HALF), bf16),
            pltpu.VMEM((2, SIDE, SIDE, 128, HALF), bf16),
            pltpu.VMEM((2, 2, STRIP, WIDTH), bf16),
            pltpu.VMEM((2, 2, 2, STRIP, WIDTH), bf16),
            pltpu.VMEM((2, 2, 2, SIDE, 64, HALF), bf16),
            pltpu.VMEM((2, 2, 2, 2, SIDE, 64, HALF), bf16),
            pltpu.VMEM((2, 2, 2, 64, HALF), bf16),
            pltpu.VMEM((2, 2, 2, 2, 64, HALF), bf16),
            pltpu.SemaphoreType.DMA((8,)),
            pltpu.SemaphoreType.DMA((7,)),
            pltpu.SemaphoreType.DMA((41,)),
            pltpu.SemaphoreType.DMA((14,)),
            pltpu.SemaphoreType.DMA((32,)),
        ],
        compiler_params=pltpu.CompilerParams(
            collective_id=0, has_side_effects=True, vmem_limit_bytes=LIMIT
        ),
    )(*arrays)
    return pl.pallas_call(
        store_kernel,
        out_shape=tuple(jax.ShapeDtypeStruct(shape, kind) for shape, kind in kept),
        in_specs=[inside] * 5,
        out_specs=(anywhere,) * 5,
        scratch_shapes=[pltpu.SemaphoreType.DMA((5,))],
        compiler_params=pltpu.CompilerParams(vmem_limit_bytes=2**20),
    )(*[pltpu.with_memory_space_constraint(r, pltpu.VMEM) for r in results])


def solution(mesh):
    in_specs = (
        P("fs", "tp"),
        P("fs", "tp"),
        P("fs", "tp"),
        P("fs", "tp"),
        P("tp", "fs"),
        P("fs", "tp"),
        P("fs", "tp"),
    )
    out_specs = (P("fs", "tp"),) * 5
    return jax.shard_map(
        on_device, mesh=mesh, in_specs=in_specs, out_specs=out_specs, check_vma=False
    )
```

```python
import jax
import jax.numpy as jnp
from jax import lax
from jax.experimental import pallas as pl
from jax.experimental.pallas import tpu as pltpu
from jax.sharding import PartitionSpec as P

contract_last = (((1,), (1,)), ((), ()))
contract_first = (((0,), (0,)), ((), ()))
bf16, f32 = jnp.bfloat16, jnp.float32
MESH = pl.DeviceIdType.MESH
SIDE = 4
ROWS, WIDTH, MODEL, HIDDEN = 768, 256, 2048, 1024
HALF = HIDDEN // 2
STRIP = ROWS // 2
LIMIT = 60 * 2**20


def around(k):
    return lax.rem(k + SIDE, SIDE)


class Place:
    def __init__(self):
        fs, tp = lax.axis_index("fs"), lax.axis_index("tp")
        self.z, self.x = fs // SIDE, lax.rem(fs, SIDE)
        self.y, self.core = tp // 2, lax.rem(tp, 2)

    def device(self, z=0, x=0, y=0, core=0):
        fs = around(self.z + z) * SIDE + around(self.x + x)
        tp = around(self.y + y) * 2 + lax.rem(self.core + core, 2)
        return (fs, tp)

    def neighbours(self):
        return [self.device(**{a: d}) for a in ("z", "x", "y") for d in (1, -1)] + [
            self.device(core=1)
        ]


class Ring:
    def __init__(self, place, axis, piece, two, sems, bases, four=None):
        self.sems, self.two, self.four = sems, two, four
        self.last = 2 if four is None else 1
        self.base = bases[0]
        del bases[: self.last + 1]
        at = getattr(place, axis)
        on, back = place.device(**{axis: 1}), place.device(**{axis: -1})
        before, after, across = around(at - 1), around(at + 1), around(at + 2)
        self.sent = [
            (piece(at, 0), on),
            (piece(at, 1), on),
            (piece(at, 1), back),
            (piece(at, 0), back),
            (piece(before, 0), on),
            (piece(after, 1), back),
        ]

    def copy(self, j, ref):
        send, receive = self.sems
        return pltpu.make_async_remote_copy(
            src_ref=ref,
            dst_ref=ref,
            send_sem=send,
            recv_sem=receive.at[self.base + (0, 1, 0, 1, self.last, self.last)[j]],
            device_id=self.sent[j][1],
            device_id_type=MESH,
        )

    def start(self, *which):
        for j in which:
            self.copy(j, self.sent[j][0]).start()

    def arrive(self, j):
        self.copy(j, self.two).wait_recv()

    def own(self):
        self.start(0, 2, 1, 3)

    def forward(self):
        self.arrive(0)
        self.start(4, 5)

    def near(self):
        self.arrive(1)

    def far(self):
        self.arrive(4)

    def rest(self):
        self.copy(1, self.four).wait_recv()


class Partner:
    def __init__(self, place, block, three, sems, base):
        self.sems, self.base, self.three = sems, base, three
        self.device = place.device(core=1)
        steps = (0, -1, 1, 2)
        self.sent = [block(around(place.y + d), place.core) for d in steps]

    def copy(self, j, ref):
        send, receive = self.sems
        return pltpu.make_async_remote_copy(
            src_ref=ref,
            dst_ref=ref,
            send_sem=send,
            recv_sem=receive.at[self.base + j // 3],
            device_id=self.device,
            device_id_type=MESH,
        )

    def start(self, *which):
        for j in which:
            self.copy(j, self.sent[j]).start()

    def most(self):
        self.copy(0, self.three).wait_recv()

    def last(self):
        self.copy(3, self.sent[3]).wait_recv()


class RingSum:
    def __init__(self, place, axis, block, far, near, sems, base):
        self.sems, self.base = sems, base
        self.both_far, self.both_near = far(slice(None)), near(slice(None), slice(None))
        at = getattr(place, axis)
        on, back = place.device(**{axis: 1}), place.device(**{axis: -1})
        before, after, across = around(at - 1), around(at + 1), around(at + 2)
        self.mine = [block(at, s) for s in range(2)]
        self.far, self.near = far, near
        self.sent = [
            (block(across, 0), far(0), on),
            (block(across, 1), far(1), back),
            (block(after, 1), near(0, 1), on),
            (block(before, 0), near(1, 0), back),
            (block(after, 0), near(0, 0), on),
            (block(before, 1), near(1, 1), back),
        ]

    def copy(self, j):
        send, receive = self.sems
        src, dst, device = self.sent[j]
        return pltpu.make_async_remote_copy(
            src_ref=src,
            dst_ref=dst,
            send_sem=send,
            recv_sem=receive.at[self.base + (0, 0, 1, 1, 1, 1)[j]],
            device_id=device,
            device_id_type=MESH,
        )

    def start(self, *which):
        for j in which:
            self.copy(j).start()

    def begin(self):
        self.start(0, 1, 2, 3)

    def receive(self, ref, k):
        send, receive = self.sems
        pltpu.make_async_remote_copy(
            src_ref=ref,
            dst_ref=ref,
            send_sem=send,
            recv_sem=receive.at[self.base + k],
            device_id=self.sent[0][2],
            device_id_type=MESH,
        ).wait_recv()

    def middle(self):
        self.receive(self.both_far, 0)
        for j in range(2):
            ref = self.sent[4 + j][0]
            ref[...] = (ref[...].astype(f32) + self.far(j)[...].astype(f32)).astype(bf16)
        self.start(4, 5)

    def total(self, s):
        return (
            self.mine[s][...].astype(f32)
            + self.near(0, s)[...].astype(f32)
            + self.near(1, s)[...].astype(f32)
        )

    def arrive(self):
        self.receive(self.both_near, 1)

    def finish(self, result=None):
        self.arrive()
        for s in range(2):
            target = self.mine[s] if result is None else result.at[pl.ds(s * STRIP, STRIP), :]
            target[...] = self.total(s).astype(bf16)


def dot(a, b):
    return jnp.dot(a, b, preferred_element_type=f32)


def dot_turned(a, b):
    return lax.dot_general(a, b, contract_last, preferred_element_type=f32)


def layer_kernel(
    factor,
    later_in, earlier_in, cot_in, up_in, down_in, up_run_in, down_run_in,
    later_out_ref, pre, back_out, up_run, down_run,
    act, turned, up, down, first_up, hidden, early_hidden, grad, part, other, up_sum, down_sum,
    far_row, near_row, far_one, near_one, far_two, near_two,
    load_sem, send_sem, ring_recv, pair_recv, sum_recv,
):
    place = Place()
    barrier = pltpu.get_barrier_semaphore()
    for neighbour in place.neighbours():
        pl.semaphore_signal(barrier, inc=1, device_id=neighbour, device_id_type=MESH)

    def act_at(a, y, core, first, count):
        column = pl.multiple_of((y * 2 + core) * WIDTH, WIDTH)
        return act.at[a, pl.ds(first, count), pl.ds(column, WIDTH)]

    def down_at(h, s, first, count):
        return down.at[pl.ds(h * HALF + s * 256, 256), pl.ds(pl.multiple_of(first * 128, 128), count)]

    here = place.z * SIDE + place.x
    loads = [(up_in.at[:, pl.ds(h * HALF, HALF)], up.at[h, place.z, place.x]) for h in range(2)]
    loads.insert(1, (down_in, down.at[:, pl.ds(pl.multiple_of(here * 128, 128), 128)]))
    for a, ref in enumerate((earlier_in, cot_in, later_in)):
        loads.insert(2 + 2 * a, (ref, act_at(a, place.y, place.core, 0, ROWS)))
    loads += [(up_run_in, up_run), (down_run_in, down_run)]
    loads = [pltpu.make_async_copy(s, d, load_sem.at[i]) for i, (s, d) in enumerate(loads)]
    for load in loads:
        load.start()

    sems, block, pair = (send_sem.at[0], ring_recv), up.at[0, 0, 0], up.at[0, 0, pl.ds(0, 2)]
    rings = list(range(41))
    rows = [
        Ring(place, "y", lambda k, s, a=a: act_at(a, k, place.core, s * 384, 384), act.at[a, :, pl.ds(0, WIDTH)],
            (send_sem.at[6], ring_recv), rings)
        for a in range(3)
    ]
    pairs = [
        Partner(place, lambda y, c, a=a: act_at(a, y, c, 0, ROWS), act.at[a, :, pl.ds(0, 3 * WIDTH)], (send_sem.at[1], pair_recv), 2 * a)
        for a in range(3)
    ]
    first, second = [], []
    for h in range(2):
        first.append((
            Ring(place, "z", lambda k, s, h=h: up.at[h, k, place.x, pl.ds(s * 64, 64), :], block, sems, rings),
            Ring(place, "x", lambda k, s, h=h: down_at(h, s, place.z * SIDE + k, 128), block, sems, rings),
        ))
    for d in (0, -1, 1, 2):
        z, x = around(place.z + d), around(place.x + d)
        second.append((
            Ring(place, "x", lambda k, s, z=z: up.at[0, z, k, pl.ds(s * 64, 64), :], block, sems, rings, pair),
            Ring(place, "z", lambda k, s, x=x: down_at(0, s, k * SIDE + x, 128), block, sems, rings, pair),
        ))
    last = (
        Ring(place, "x", lambda k, s: up.at[1, :, k, pl.ds(s * 64, 64), :], up.at[0, 0], sems, rings, up.at[0, pl.ds(0, 2)]),
        Ring(place, "z", lambda k, s: down_at(1, s, k * SIDE, 512), up.at[0, 0], sems, rings, up.at[0, pl.ds(0, 2)]),
    )

    sums = iter(range(0, 32, 2))
    row_sums = [
        RingSum(
            place, "y", lambda k, s, a=a: part.at[a, place.core, k, pl.ds(s * 384, 384), :],
            lambda d, a=a: far_row.at[a, d], lambda d, s, a=a: near_row.at[a, d, s], (send_sem.at[2], sum_recv), next(sums),
        )
        for a in range(2)
    ]
    one, two = (send_sem.at[3], sum_recv), (send_sem.at[4], sum_recv)
    first_sums = (
        RingSum(
            place, "z", lambda k, s: down_sum.at[0, k, :, pl.ds(s * 64, 64), :],
            lambda d: far_one.at[1, 0, d], lambda d, s: near_one.at[1, 0, d, s], one, next(sums),
        ),
        RingSum(
            place, "x", lambda k, s: up_sum.at[0, :, k, pl.ds(s * 64, 64), :],
            lambda d: far_one.at[0, 0, d], lambda d, s: near_one.at[0, 0, d, s], one, next(sums),
        ),
    )
    down_lines, up_lines, second_sums = [], [], []
    for q in (2, 1, -1, 0):
        z, x = around(place.z + q), around(place.x + q)
        down_lines.append(RingSum(
            place, "z", lambda k, s, x=x: down_sum.at[1, k, x, pl.ds(s * 64, 64), :],
            lambda d, x=x: far_one.at[1, 1, d, x], lambda d, s, x=x: near_one.at[1, 1, d, s, x], one, next(sums),
        ))
        up_lines.append(RingSum(
            place, "x", lambda k, s, z=z: up_sum.at[1, z, k, pl.ds(s * 64, 64), :],
            lambda d, z=z: far_one.at[0, 1, d, z], lambda d, s, z=z: near_one.at[0, 1, d, s, z], one, next(sums),
        ))
    lines = list(zip(down_lines, up_lines))
    for h in range(2):
        second_sums.append((
            RingSum(
                place, "x", lambda k, s, h=h: down_sum.at[h, place.z, k, pl.ds(s * 64, 64), :],
                lambda d, h=h: far_two.at[1, h, d], lambda d, s, h=h: near_two.at[1, h, d, s], two, next(sums),
            ),
            RingSum(
                place, "z", lambda k, s, h=h: up_sum.at[h, k, place.x, pl.ds(s * 64, 64), :],
                lambda d, h=h: far_two.at[0, h, d], lambda d, s, h=h: near_two.at[0, h, d, s], two, next(sums),
            ),
        ))

    order = [around(place.y + d) for d in (2, 1, -1, 0)]

    def swap(a, i):
        return pltpu.make_async_remote_copy(
            src_ref=part.at[a, 1 - place.core, order[i]],
            dst_ref=other.at[a, order[i]],
            send_sem=send_sem.at[5],
            recv_sem=pair_recv.at[6 + 4 * a + i],
            device_id=place.device(core=1),
            device_id_type=MESH,
        )

    def sent(i, ref):
        pltpu.make_async_remote_copy(
            src_ref=ref,
            dst_ref=ref,
            send_sem=send_sem.at[i],
            recv_sem=pair_recv.at[0],
            device_id=place.device(core=1),
            device_id_type=MESH,
        ).wait_send()

    def both(stage, name):
        for ring in stage:
            getattr(ring, name)()

    def strip(m):
        return pl.ds(pl.multiple_of(m * STRIP, STRIP), STRIP)

    def columns(h):
        return pl.ds(h * HALF, HALF)

    def turn(a, core, start, stop):
        @pl.loop(start, stop)
        def _(d):
            block = pl.ds(pl.multiple_of((around(place.y + d) * 2 + core) * WIDTH, WIDTH), WIDTH)
            turned[a, block, :] = act[a, :, block].T

    def up_of(h):
        return up[h].reshape(MODEL, HALF)

    def earlier_up(h):
        @pl.loop(0, 2)
        def _(m):
            value = jnp.maximum(dot(act[0, strip(m), :], up_of(h)), 0.0)
            first_up[strip(m), :] = value
            early_hidden[strip(m), columns(h)] = jnp.square(value).astype(bf16)

    def hidden_grad(h):
        @pl.loop(0, 2)
        def _(m):
            value = dot_turned(act[1, strip(m), :], down[columns(h), :])
            grad[strip(m), columns(h)] = (2.0 * first_up[strip(m), :] * value).astype(bf16)

    def weight_grad(a, source, target, h):
        @pl.loop(0, 4)
        def _(n):
            block = pl.ds(pl.multiple_of(n * 512, 512), 512)
            value = dot(turned[a, block, :], source[:, columns(h)])
            target[h, n] = value.astype(bf16).reshape(SIDE, 128, HALF)

    def later_up(h):
        @pl.loop(0, 2)
        def _(m):
            value = dot(act[2, strip(m), :], up_of(h))
            pre[strip(m), columns(h)] = value.astype(bf16)
            hidden[strip(m), columns(h)] = jnp.square(jnp.maximum(value, 0.0)).astype(bf16)

    def keep(a, n, m, value):
        value = value.astype(bf16)
        part[a, 0, n, strip(m), :] = value[:, :WIDTH]
        part[a, 1, n, strip(m), :] = value[:, WIDTH:]

    def later_out(i):
        n = order[i]
        block = pl.ds(pl.multiple_of(n * 512, 512), 512)

        @pl.loop(0, 2)
        def _(m):
            keep(0, n, m, dot(hidden[strip(m), :], down[:, block]))

        swap(0, i).start()

    def input_grad(i):
        n = order[i]

        @pl.loop(0, 2)
        def _(m):
            weight = jnp.concatenate([up[h, n].reshape(512, HALF) for h in range(2)], axis=1)
            keep(1, n, m, dot_turned(grad[strip(m), :], weight))

        swap(1, i).start()

    def join(a, i):
        swap(a, i).wait_recv()
        n = order[i]
        part[a, place.core, n] = (
            part[a, place.core, n].astype(f32) + other[a, n].astype(f32)
        ).astype(bf16)
        row_sums[a].start(*((0, 1), (2,), (3,), ())[i])

    def add_running(w, ring, h):
        ring.arrive()
        for s in range(2):
            at = (up_run, down_run)[w].at[pl.ds(s * 64, 64), columns(h)]
            at[...] = at[...] + ring.total(s) * factor

    pl.semaphore_wait(barrier, 7)
    loads[0].wait()
    loads[1].wait()

    both(first[0], "own")
    both(second[0], "own")
    loads[2].wait()
    rows[0].own()
    pairs[0].start(0)
    for load in loads[3:]:
        load.wait()
    both(first[0], "forward")
    both(first[1], "own")
    both(first[0], "near")
    both(second[1], "own")
    both(second[2], "own")
    both(second[0], "forward")
    rows[0].forward()
    rows[1].own()
    pairs[1].start(0)
    both(first[0], "far")
    both(second[3], "own")
    both(first[1], "forward")
    both(second[1], "forward")
    rows[0].near()
    pairs[0].start(1, 2)
    rows[0].far()
    pairs[0].start(3)
    both(second[2], "forward")
    both(second[3], "forward")
    rows[1].forward()
    rows[2].own()
    pairs[2].start(0)
    both(first[1], "near")
    both(first[1], "far")
    both(last, "own")
    pairs[0].most()
    pairs[0].last()
    turn(0, place.core, -1, 3)
    turn(0, 1 - place.core, -1, 3)
    rows[1].near()
    pairs[1].start(1, 2)
    for ring in second:
        both(ring, "rest")
    earlier_up(0)
    rows[1].far()
    pairs[1].start(3)
    turn(1, place.core, -1, 3)
    pairs[1].most()
    turn(1, 1 - place.core, -1, 2)
    pairs[1].last()
    turn(1, 1 - place.core, 2, 3)
    rows[2].forward()
    both(last, "forward")
    weight_grad(1, early_hidden, down_sum, 0)
    first_sums[0].begin()
    hidden_grad(0)
    rows[2].near()
    pairs[2].start(1, 2)
    weight_grad(0, grad, up_sum, 0)
    first_sums[1].begin()
    rows[2].far()
    pairs[2].start(3)
    pairs[2].most()
    pairs[2].last()
    later_up(0)
    both(last, "rest")
    earlier_up(1)
    hidden_grad(1)
    input_grad(0)
    input_grad(1)
    both(first_sums, "middle")
    weight_grad(1, early_hidden, down_sum, 1)
    both(down_lines[:3], "begin")
    join(1, 0)
    weight_grad(0, grad, up_sum, 1)
    both(up_lines[:3], "begin")
    join(1, 1)
    input_grad(2)
    input_grad(3)
    later_up(1)
    join(1, 2)
    join(1, 3)
    both(first_sums, "finish")
    both(second_sums[0], "begin")
    row_sums[1].middle()
    later_out(0)
    later_out(1)
    later_out(2)
    join(0, 0)
    later_out(3)
    join(0, 1)
    for line in lines[:3]:
        both(line, "middle")
    both(lines[3], "begin")
    both(second_sums[0], "middle")
    join(0, 2)
    join(0, 3)
    row_sums[1].finish(back_out)
    both(lines[0], "finish")
    for ring in second_sums[1]:
        ring.start(0, 1)
    row_sums[0].middle()
    both(lines[1], "finish")
    both(lines[2], "finish")
    for ring in second_sums[1]:
        ring.start(2, 3)
    both(lines[3], "middle")
    both(second_sums[1], "middle")
    add_running(1, second_sums[0][0], 0)
    add_running(0, second_sums[0][1], 0)
    row_sums[0].finish(later_out_ref)
    both(lines[3], "finish")
    add_running(1, second_sums[1][0], 1)
    add_running(0, second_sums[1][1], 1)
    sent(0, act.at[:, pl.ds(0, 640), :])
    sent(1, act.at[:, pl.ds(0, 384), :])
    sent(2, act.at[0, pl.ds(0, 576), :])
    sent(3, act.at[pl.ds(0, 2)])
    sent(4, act.at[0, pl.ds(0, 384), :])
    sent(5, act.at[0])
    sent(6, act.at[pl.ds(0, 2), pl.ds(0, 432), :])


def store_kernel(*refs):
    sources, results, sem = refs[:5], refs[5:10], refs[10]
    copies = [
        pltpu.make_async_copy(src, dst, sem.at[i]) for i, (src, dst) in enumerate(zip(sources, results))
    ]
    for copy in copies:
        copy.start()
    for copy in copies:
        copy.wait()


def on_device(*arrays):
    factor = float(ROWS * 16) ** (-0.5)
    anywhere = pl.BlockSpec(memory_space=pl.ANY)
    inside = pl.BlockSpec(memory_space=pltpu.VMEM)
    kept = [
        ((ROWS, WIDTH), bf16),
        ((ROWS, HIDDEN), bf16),
        ((ROWS, WIDTH), bf16),
        ((128, HIDDEN), f32),
        ((128, HIDDEN), f32),
    ]
    results = pl.pallas_call(
        lambda *refs: layer_kernel(factor, *refs),
        out_shape=tuple(pltpu.VMEM(shape, kind) for shape, kind in kept),
        in_specs=[anywhere] * 7,
        out_specs=(inside,) * 5,
        scratch_shapes=[
            pltpu.VMEM((3, ROWS, MODEL), bf16),
            pltpu.VMEM((2, MODEL, ROWS), bf16),
            pltpu.VMEM((2, SIDE, SIDE, 128, HALF), bf16),
            pltpu.VMEM((HIDDEN, MODEL), bf16),
            pltpu.VMEM((ROWS, HALF), f32),
            pltpu.VMEM((ROWS, HIDDEN), bf16),
            pltpu.VMEM((ROWS, HIDDEN), bf16),
            pltpu.VMEM((ROWS, HIDDEN), bf16),
            pltpu.VMEM((2, 2, SIDE, ROWS, WIDTH), bf16),
            pltpu.VMEM((2, SIDE, ROWS, WIDTH), bf16),
            pltpu.VMEM((2, SIDE, SIDE, 128, HALF), bf16),
            pltpu.VMEM((2, SIDE, SIDE, 128, HALF), bf16),
            pltpu.VMEM((2, 2, STRIP, WIDTH), bf16),
            pltpu.VMEM((2, 2, 2, STRIP, WIDTH), bf16),
            pltpu.VMEM((2, 2, 2, SIDE, 64, HALF), bf16),
            pltpu.VMEM((2, 2, 2, 2, SIDE, 64, HALF), bf16),
            pltpu.VMEM((2, 2, 2, 64, HALF), bf16),
            pltpu.VMEM((2, 2, 2, 2, 64, HALF), bf16),
            pltpu.SemaphoreType.DMA((8,)),
            pltpu.SemaphoreType.DMA((7,)),
            pltpu.SemaphoreType.DMA((41,)),
            pltpu.SemaphoreType.DMA((14,)),
            pltpu.SemaphoreType.DMA((32,)),
        ],
        compiler_params=pltpu.CompilerParams(
            collective_id=0, has_side_effects=True, vmem_limit_bytes=LIMIT
        ),
    )(*arrays)
    return pl.pallas_call(
        store_kernel,
        out_shape=tuple(jax.ShapeDtypeStruct(shape, kind) for shape, kind in kept),
        in_specs=[inside] * 5,
        out_specs=(anywhere,) * 5,
        scratch_shapes=[pltpu.SemaphoreType.DMA((5,))],
        compiler_params=pltpu.CompilerParams(vmem_limit_bytes=2**20),
    )(*[pltpu.with_memory_space_constraint(r, pltpu.VMEM) for r in results])


def solution(mesh):
    in_specs = (
        P("fs", "tp"),
        P("fs", "tp"),
        P("fs", "tp"),
        P("fs", "tp"),
        P("tp", "fs"),
        P("fs", "tp"),
        P("fs", "tp"),
    )
    out_specs = (P("fs", "tp"),) * 5
    return jax.shard_map(
        on_device, mesh=mesh, in_specs=in_specs, out_specs=out_specs, check_vma=False
    )
```

```python
import jax
import jax.numpy as jnp
from jax import lax
from jax.experimental import pallas as pl
from jax.experimental.pallas import tpu as pltpu
from jax.sharding import PartitionSpec as P

contract_last = (((1,), (1,)), ((), ()))
contract_first = (((0,), (0,)), ((), ()))
bf16, f32 = jnp.bfloat16, jnp.float32
MESH = pl.DeviceIdType.MESH
SIDE = 4
ROWS, WIDTH, MODEL, HIDDEN = 768, 256, 2048, 1024
HALF = HIDDEN // 2
STRIP = ROWS // 2
LIMIT = 60 * 2**20


def around(k):
    return lax.rem(k + SIDE, SIDE)


class Place:
    def __init__(self):
        fs, tp = lax.axis_index("fs"), lax.axis_index("tp")
        self.z, self.x = fs // SIDE, lax.rem(fs, SIDE)
        self.y, self.core = tp // 2, lax.rem(tp, 2)

    def device(self, z=0, x=0, y=0, core=0):
        fs = around(self.z + z) * SIDE + around(self.x + x)
        tp = around(self.y + y) * 2 + lax.rem(self.core + core, 2)
        return (fs, tp)

    def neighbours(self):
        return [self.device(**{a: d}) for a in ("z", "x", "y") for d in (1, -1)] + [
            self.device(core=1)
        ]


def remote(src, dst, device, send, receive):
    return pltpu.make_async_remote_copy(
        src_ref=src, dst_ref=dst, send_sem=send, recv_sem=receive, device_id=device, device_id_type=MESH
    )


class Ring:
    def __init__(self, place, parts, half, bulk, sems, bases, joint=False):
        self.place, self.count, self.bulk, self.sems = place, half * len(parts), bulk, sems
        self.last = 1 if joint else 2
        self.base = bases[0]
        del bases[: self.last + 1]
        self.sent = []
        for axis, piece in parts:
            at = getattr(place, axis)
            on, back = place.device(**{axis: 1}), place.device(**{axis: -1})
            before, after = around(at - 1), around(at + 1)
            self.sent.append([
                (piece(at, 0), on),
                (piece(at, 1), on),
                (piece(at, 1), back),
                (piece(at, 0), back),
                (piece(before, 0), on),
                (piece(after, 1), back),
            ])

    def start(self, *which):
        send, receive = self.sems
        for part in self.sent:
            for j in which:
                ref, device = part[j]
                k = (0, 1, 0, 1, self.last, self.last)[j]
                remote(ref, ref, device, send, receive.at[self.base + k]).start()

    def wait(self, k, halves):
        send, receive = self.sems
        ref = self.bulk(halves * self.count)
        remote(ref, ref, self.place.device(core=1), send, receive.at[self.base + k]).wait_recv()

    def own(self):
        self.start(0, 2, 1, 3)

    def forward(self):
        self.wait(0, 2)
        self.start(4, 5)

    def near(self):
        self.wait(1, 2)

    def far(self):
        self.wait(2, 2)

    def rest(self):
        self.wait(1, 4)


class Partner:
    def __init__(self, place, block, bulk, sems, base, joint):
        self.bulk, self.sems, self.base = bulk, sems, base
        self.keys = (0, 0, 0, 0) if joint else (0, 0, 0, 1)
        self.device = place.device(core=1)
        self.sent = [block(around(place.y + d), place.core) for d in (0, -1, 1, 2)]

    def start(self, *which):
        send, receive = self.sems
        for j in which:
            ref = self.sent[j]
            remote(ref, ref, self.device, send, receive.at[self.base + self.keys[j]]).start()

    def wait(self, k, blocks):
        send, receive = self.sems
        ref = self.bulk(blocks * ROWS * WIDTH)
        remote(ref, ref, self.device, send, receive.at[self.base + k]).wait_recv()


class RingSum:
    def __init__(self, place, parts, half, bulk, sems, base):
        self.place, self.count, self.bulk, self.sems, self.base = place, half * len(parts), bulk, sems, base
        self.mine, self.boxes, self.sent = [], [], []
        for axis, block, far, near in parts:
            at = getattr(place, axis)
            on, back = place.device(**{axis: 1}), place.device(**{axis: -1})
            before, after, across = around(at - 1), around(at + 1), around(at + 2)
            self.mine.append([block(at, s) for s in range(2)])
            self.boxes.append((far, near))
            self.sent.append([
                (block(across, 0), far(0), on),
                (block(across, 1), far(1), back),
                (block(after, 1), near(0, 1), on),
                (block(before, 0), near(1, 0), back),
                (block(after, 0), near(0, 0), on),
                (block(before, 1), near(1, 1), back),
            ])

    def start(self, which, parts=None):
        send, receive = self.sems
        for part in self.sent if parts is None else [self.sent[p] for p in parts]:
            for j in which:
                src, dst, device = part[j]
                remote(src, dst, device, send, receive.at[self.base + (0 if j < 2 else 1)]).start()

    def begin(self, *parts):
        self.start((0, 1, 2, 3), parts or None)

    def wait(self, k, halves):
        send, receive = self.sems
        ref = self.bulk(halves * self.count)
        remote(ref, ref, self.place.device(core=1), send, receive.at[self.base + k]).wait_recv()

    def middle(self):
        self.wait(0, 2)
        for p, (far, near) in enumerate(self.boxes):
            for j in range(2):
                ref = self.sent[p][4 + j][0]
                ref[...] = (ref[...].astype(f32) + far(j)[...].astype(f32)).astype(bf16)
            self.start((4, 5), (p,))

    def arrive(self):
        self.wait(1, 4)

    def total(self, p, s):
        near = self.boxes[p][1]
        return (
            self.mine[p][s][...].astype(f32)
            + near(0, s)[...].astype(f32)
            + near(1, s)[...].astype(f32)
        )

    def finish(self, result=None):
        self.arrive()
        for p, mine in enumerate(self.mine):
            for s in range(2):
                target = mine[s] if result is None else result.at[pl.ds(s * STRIP, STRIP), :]
                target[...] = self.total(p, s).astype(bf16)


def dot(a, b):
    return jnp.dot(a, b, preferred_element_type=f32)


def dot_turned(a, b):
    return lax.dot_general(a, b, contract_last, preferred_element_type=f32)


def layer_kernel(
    factor,
    later_in, earlier_in, cot_in, up_in, down_in, up_run_in, down_run_in,
    later_out_ref, pre, back_out, up_run, down_run,
    act, turned, up, down, first_up, hidden, early_hidden, grad, part, other, up_sum, down_sum,
    far_row, near_row, far_one, near_one, far_two, near_two,
    load_sem, send_sem, ring_recv, pair_recv, sum_recv,
):
    place = Place()
    barrier = pltpu.get_barrier_semaphore()
    for neighbour in place.neighbours():
        pl.semaphore_signal(barrier, inc=1, device_id=neighbour, device_id_type=MESH)

    def act_at(a, y, core, first, count):
        column = pl.multiple_of((y * 2 + core) * WIDTH, WIDTH)
        return act.at[a, pl.ds(first, count), pl.ds(column, WIDTH)]

    def down_at(h, s, first, count):
        return down.at[pl.ds(h * HALF + s * 256, 256), pl.ds(pl.multiple_of(first * 128, 128), count)]

    def bulk(count):
        return act.at[0, pl.ds(0, count // MODEL), :]

    here = place.z * SIDE + place.x
    mine = [act_at(a, place.y, place.core, 0, ROWS) for a in range(3)]
    loads = [
        (up_in.at[:, pl.ds(0, HALF)], up.at[0, place.z, place.x], 0),
        (down_in, down.at[:, pl.ds(pl.multiple_of(here * 128, 128), 128)], 0),
        (earlier_in, mine[0], 1),
        (up_in.at[:, pl.ds(HALF, HALF)], up.at[1, place.z, place.x], 2),
        (cot_in, mine[1], 2),
        (later_in, mine[2], 2),
        (up_run_in, up_run, 2),
        (down_run_in, down_run, 2),
    ]
    for src, dst, k in loads:
        pltpu.make_async_copy(src, dst, load_sem.at[k]).start()

    def loaded(k, count):
        ref = bulk(count)
        pltpu.make_async_copy(ref, ref, load_sem.at[k]).wait()

    bases = list(range(24))
    sems = (send_sem.at[0], ring_recv)
    rows = [
        Ring(
            place, [("y", lambda k, s, a=a: act_at(a, k, place.core, s * STRIP, STRIP))],
            STRIP * WIDTH, bulk, (send_sem.at[2], ring_recv), bases,
        )
        for a in range(3)
    ]
    pairs = [
        Partner(
            place, lambda y, c, a=a: act_at(a, y, c, 0, ROWS), bulk, (send_sem.at[2], pair_recv),
            (0, 1, 3)[a], a != 1,
        )
        for a in range(3)
    ]
    first, second = [], []
    for h in range(2):
        first.append(Ring(
            place,
            [
                ("z", lambda k, s, h=h: up.at[h, k, place.x, pl.ds(s * 64, 64), :]),
                ("x", lambda k, s, h=h: down_at(h, s, place.z * SIDE + k, 128)),
            ],
            64 * HALF, bulk, sems, bases, h == 1,
        ))
    for d in (0, -1, 1, 2):
        z, x = around(place.z + d), around(place.x + d)
        second.append(Ring(
            place,
            [
                ("x", lambda k, s, z=z: up.at[0, z, k, pl.ds(s * 64, 64), :]),
                ("z", lambda k, s, x=x: down_at(0, s, k * SIDE + x, 128)),
            ],
            64 * HALF, bulk, sems, bases, True,
        ))
    last = Ring(
        place,
        [
            ("x", lambda k, s: up.at[1, :, k, pl.ds(s * 64, 64), :]),
            ("z", lambda k, s: down_at(1, s, k * SIDE, 512)),
        ],
        SIDE * 64 * HALF, bulk, sems, bases, True,
    )

    sums = iter(range(0, 18, 2))
    row_sums = [
        RingSum(
            place,
            [(
                "y", lambda k, s, a=a: part.at[a, place.core, k, pl.ds(s * STRIP, STRIP), :],
                lambda d, a=a: far_row.at[a, d], lambda d, s, a=a: near_row.at[a, d, s],
            )],
            STRIP * WIDTH, bulk, (send_sem.at[3], sum_recv), next(sums),
        )
        for a in range(2)
    ]
    sems = (send_sem.at[1], sum_recv)
    first_sum = RingSum(
        place,
        [
            (
                "z", lambda k, s: down_sum.at[0, k, :, pl.ds(s * 64, 64), :],
                lambda d: far_one.at[1, 0, d], lambda d, s: near_one.at[1, 0, d, s],
            ),
            (
                "x", lambda k, s: up_sum.at[0, :, k, pl.ds(s * 64, 64), :],
                lambda d: far_one.at[0, 0, d], lambda d, s: near_one.at[0, 0, d, s],
            ),
        ],
        SIDE * 64 * HALF, bulk, sems, next(sums),
    )
    lines, second_sums = [], []
    for q in (2, 1, -1, 0):
        z, x = around(place.z + q), around(place.x + q)
        lines.append(RingSum(
            place,
            [
                (
                    "z", lambda k, s, x=x: down_sum.at[1, k, x, pl.ds(s * 64, 64), :],
                    lambda d, x=x: far_one.at[1, 1, d, x], lambda d, s, x=x: near_one.at[1, 1, d, s, x],
                ),
                (
                    "x", lambda k, s, z=z: up_sum.at[1, z, k, pl.ds(s * 64, 64), :],
                    lambda d, z=z: far_one.at[0, 1, d, z], lambda d, s, z=z: near_one.at[0, 1, d, s, z],
                ),
            ],
            64 * HALF, bulk, sems, next(sums),
        ))
    for h in range(2):
        second_sums.append(RingSum(
            place,
            [
                (
                    "x", lambda k, s, h=h: down_sum.at[h, place.z, k, pl.ds(s * 64, 64), :],
                    lambda d, h=h: far_two.at[1, h, d], lambda d, s, h=h: near_two.at[1, h, d, s],
                ),
                (
                    "z", lambda k, s, h=h: up_sum.at[h, k, place.x, pl.ds(s * 64, 64), :],
                    lambda d, h=h: far_two.at[0, h, d], lambda d, s, h=h: near_two.at[0, h, d, s],
                ),
            ],
            64 * HALF, bulk, sems, next(sums),
        ))

    order = [around(place.y + d) for d in (2, 1, -1, 0)]

    def swap(a, i):
        return remote(
            part.at[a, 1 - place.core, order[i]], other.at[a, order[i]], place.device(core=1),
            send_sem.at[3], pair_recv.at[4 + 3 * a + (0, 1, 2, 2)[i]],
        )

    def sent(i, count):
        ref = act.at[:, pl.ds(0, count // (3 * MODEL)), :]
        remote(ref, ref, place.device(core=1), send_sem.at[i], pair_recv.at[0]).wait_send()

    def strip(m):
        return pl.ds(pl.multiple_of(m * STRIP, STRIP), STRIP)

    def columns(h):
        return pl.ds(h * HALF, HALF)

    def turn(a, core, start, stop):
        @pl.loop(start, stop)
        def _(d):
            block = pl.ds(pl.multiple_of((around(place.y + d) * 2 + core) * WIDTH, WIDTH), WIDTH)
            turned[a, block, :] = act[a, :, block].T

    def up_of(h):
        return up[h].reshape(MODEL, HALF)

    def earlier_up(h):
        @pl.loop(0, 2)
        def _(m):
            value = jnp.maximum(dot(act[0, strip(m), :], up_of(h)), 0.0)
            first_up[strip(m), :] = value
            early_hidden[strip(m), columns(h)] = jnp.square(value).astype(bf16)

    def hidden_grad(h):
        @pl.loop(0, 2)
        def _(m):
            value = dot_turned(act[1, strip(m), :], down[columns(h), :])
            grad[strip(m), columns(h)] = (2.0 * first_up[strip(m), :] * value).astype(bf16)

    def weight_grad(a, source, target, h):
        @pl.loop(0, 4)
        def _(n):
            block = pl.ds(pl.multiple_of(n * 512, 512), 512)
            value = dot(turned[a, block, :], source[:, columns(h)])
            target[h, n] = value.astype(bf16).reshape(SIDE, 128, HALF)

    def later_up(h):
        @pl.loop(0, 2)
        def _(m):
            value = dot(act[2, strip(m), :], up_of(h))
            pre[strip(m), columns(h)] = value.astype(bf16)
            hidden[strip(m), columns(h)] = jnp.square(jnp.maximum(value, 0.0)).astype(bf16)

    def keep(a, n, m, value):
        value = value.astype(bf16)
        part[a, 0, n, strip(m), :] = value[:, :WIDTH]
        part[a, 1, n, strip(m), :] = value[:, WIDTH:]

    def later_out(i):
        n = order[i]
        block = pl.ds(pl.multiple_of(n * 512, 512), 512)

        @pl.loop(0, 2)
        def _(m):
            keep(0, n, m, dot(hidden[strip(m), :], down[:, block]))

        swap(0, i).start()

    def input_grad(i):
        n = order[i]

        @pl.loop(0, 2)
        def _(m):
            weight = jnp.concatenate([up[h, n].reshape(512, HALF) for h in range(2)], axis=1)
            keep(1, n, m, dot_turned(grad[strip(m), :], weight))

        swap(1, i).start()

    def join(a, i):
        if i == 2:
            ref = bulk(2 * ROWS * WIDTH)
            remote(ref, ref, place.device(core=1), send_sem.at[3], pair_recv.at[6 + 3 * a]).wait_recv()
        elif i < 2:
            swap(a, i).wait_recv()
        n = order[i]
        part[a, place.core, n] = (
            part[a, place.core, n].astype(f32) + other[a, n].astype(f32)
        ).astype(bf16)
        row_sums[a].start(((0, 1), (2,), (3,), ())[i])

    def add_running(h):
        second_sums[h].arrive()
        for p, run in enumerate((down_run, up_run)):
            for s in range(2):
                at = run.at[pl.ds(s * 64, 64), columns(h)]
                at[...] = at[...] + second_sums[h].total(p, s) * factor

    pl.semaphore_wait(barrier, 7)
    loaded(0, 128 * HALF + HIDDEN * 128)

    first[0].own()
    second[0].own()
    loaded(1, ROWS * WIDTH)
    rows[0].own()
    pairs[0].start(0)
    loaded(2, 128 * HALF + 2 * ROWS * WIDTH + 4 * 128 * HIDDEN)
    first[0].forward()
    first[1].own()
    first[0].near()
    second[1].own()
    second[2].own()
    second[0].forward()
    rows[0].forward()
    rows[1].own()
    pairs[1].start(0)
    first[0].far()
    second[3].own()
    first[1].forward()
    second[1].forward()
    rows[0].near()
    pairs[0].start(1, 2)
    rows[0].far()
    pairs[0].start(3)
    second[2].forward()
    second[3].forward()
    rows[1].forward()
    rows[2].own()
    pairs[2].start(0)
    first[1].rest()
    last.own()
    pairs[0].wait(0, 4)
    turn(0, place.core, -1, 3)
    turn(0, 1 - place.core, -1, 3)
    rows[1].near()
    pairs[1].start(1, 2)
    for ring in second:
        ring.rest()
    earlier_up(0)
    rows[1].far()
    pairs[1].start(3)
    turn(1, place.core, -1, 3)
    pairs[1].wait(0, 3)
    turn(1, 1 - place.core, -1, 2)
    pairs[1].wait(1, 1)
    turn(1, 1 - place.core, 2, 3)
    rows[2].forward()
    last.forward()
    weight_grad(1, early_hidden, down_sum, 0)
    first_sum.begin(0)
    hidden_grad(0)
    rows[2].near()
    pairs[2].start(1, 2)
    weight_grad(0, grad, up_sum, 0)
    first_sum.begin(1)
    rows[2].far()
    pairs[2].start(3)
    pairs[2].wait(0, 4)
    later_up(0)
    last.rest()
    earlier_up(1)
    hidden_grad(1)
    input_grad(0)
    input_grad(1)
    first_sum.middle()
    weight_grad(1, early_hidden, down_sum, 1)
    for which in ((0, 1), (2, 3)):
        for line in lines[:3]:
            line.start(which, (0,))
    join(1, 0)
    weight_grad(0, grad, up_sum, 1)
    for which in ((0, 1), (2, 3)):
        for line in lines[:3]:
            line.start(which, (1,))
    join(1, 1)
    input_grad(2)
    input_grad(3)
    later_up(1)
    join(1, 2)
    join(1, 3)
    first_sum.finish()
    second_sums[0].start((0, 1))
    row_sums[1].middle()
    later_out(0)
    later_out(1)
    later_out(2)
    join(0, 0)
    for line in lines[:3]:
        line.middle()
    lines[3].start((0, 1))
    second_sums[0].start((2, 3))
    later_out(3)
    join(0, 1)
    join(0, 2)
    join(0, 3)
    lines[0].finish()
    second_sums[1].start((0, 1))
    lines[3].start((2, 3))
    second_sums[0].middle()
    row_sums[1].finish(back_out)
    lines[1].finish()
    lines[2].finish()
    second_sums[1].start((2, 3))
    row_sums[0].middle()
    lines[3].middle()
    second_sums[1].middle()
    add_running(0)
    row_sums[0].finish(later_out_ref)
    lines[3].finish()
    add_running(1)
    sent(0, 120 * 64 * HALF)
    sent(1, 120 * 64 * HALF)
    sent(2, 18 * STRIP * WIDTH + 12 * ROWS * WIDTH)
    sent(3, 12 * STRIP * WIDTH + 8 * ROWS * WIDTH)


def store_kernel(*refs):
    sources, results, sem = refs[:5], refs[5:10], refs[10]
    copies = [
        pltpu.make_async_copy(src, dst, sem.at[i]) for i, (src, dst) in enumerate(zip(sources, results))
    ]
    for copy in copies:
        copy.start()
    for copy in copies:
        copy.wait()


def on_device(*arrays):
    factor = float(ROWS * 16) ** (-0.5)
    anywhere = pl.BlockSpec(memory_space=pl.ANY)
    inside = pl.BlockSpec(memory_space=pltpu.VMEM)
    kept = [
        ((ROWS, WIDTH), bf16),
        ((ROWS, HIDDEN), bf16),
        ((ROWS, WIDTH), bf16),
        ((128, HIDDEN), f32),
        ((128, HIDDEN), f32),
    ]
    results = pl.pallas_call(
        lambda *refs: layer_kernel(factor, *refs),
        out_shape=tuple(pltpu.VMEM(shape, kind) for shape, kind in kept),
        in_specs=[anywhere] * 7,
        out_specs=(inside,) * 5,
        scratch_shapes=[
            pltpu.VMEM((3, ROWS, MODEL), bf16),
            pltpu.VMEM((2, MODEL, ROWS), bf16),
            pltpu.VMEM((2, SIDE, SIDE, 128, HALF), bf16),
            pltpu.VMEM((HIDDEN, MODEL), bf16),
            pltpu.VMEM((ROWS, HALF), f32),
            pltpu.VMEM((ROWS, HIDDEN), bf16),
            pltpu.VMEM((ROWS, HIDDEN), bf16),
            pltpu.VMEM((ROWS, HIDDEN), bf16),
            pltpu.VMEM((2, 2, SIDE, ROWS, WIDTH), bf16),
            pltpu.VMEM((2, SIDE, ROWS, WIDTH), bf16),
            pltpu.VMEM((2, SIDE, SIDE, 128, HALF), bf16),
            pltpu.VMEM((2, SIDE, SIDE, 128, HALF), bf16),
            pltpu.VMEM((2, 2, STRIP, WIDTH), bf16),
            pltpu.VMEM((2, 2, 2, STRIP, WIDTH), bf16),
            pltpu.VMEM((2, 2, 2, SIDE, 64, HALF), bf16),
            pltpu.VMEM((2, 2, 2, 2, SIDE, 64, HALF), bf16),
            pltpu.VMEM((2, 2, 2, 64, HALF), bf16),
            pltpu.VMEM((2, 2, 2, 2, 64, HALF), bf16),
            pltpu.SemaphoreType.DMA((3,)),
            pltpu.SemaphoreType.DMA((4,)),
            pltpu.SemaphoreType.DMA((24,)),
            pltpu.SemaphoreType.DMA((10,)),
            pltpu.SemaphoreType.DMA((18,)),
        ],
        compiler_params=pltpu.CompilerParams(
            collective_id=0, has_side_effects=True, vmem_limit_bytes=LIMIT
        ),
    )(*arrays)
    return pl.pallas_call(
        store_kernel,
        out_shape=tuple(jax.ShapeDtypeStruct(shape, kind) for shape, kind in kept),
        in_specs=[inside] * 5,
        out_specs=(anywhere,) * 5,
        scratch_shapes=[pltpu.SemaphoreType.DMA((5,))],
        compiler_params=pltpu.CompilerParams(vmem_limit_bytes=2**20),
    )(*[pltpu.with_memory_space_constraint(r, pltpu.VMEM) for r in results])


def solution(mesh):
    in_specs = (
        P("fs", "tp"),
        P("fs", "tp"),
        P("fs", "tp"),
        P("fs", "tp"),
        P("tp", "fs"),
        P("fs", "tp"),
        P("fs", "tp"),
    )
    out_specs = (P("fs", "tp"),) * 5
    return jax.shard_map(
        on_device, mesh=mesh, in_specs=in_specs, out_specs=out_specs, check_vma=False
    )
```

```python
import jax
import jax.numpy as jnp
from jax import lax
from jax.experimental import pallas as pl
from jax.experimental.pallas import tpu as pltpu
from jax.sharding import PartitionSpec as P

contract_last = (((1,), (1,)), ((), ()))
bf16, f32 = jnp.bfloat16, jnp.float32
MESH = pl.DeviceIdType.MESH
SIDE = 4
ROWS, WIDTH, MODEL, HIDDEN = 768, 256, 2048, 1024
HALF = HIDDEN // 2
STRIP = ROWS // 2
LIMIT = 60 * 2**20


def around(k):
    return lax.rem(k + SIDE, SIDE)


class Place:
    def __init__(self):
        fs, tp = lax.axis_index("fs"), lax.axis_index("tp")
        self.z, self.x = fs // SIDE, lax.rem(fs, SIDE)
        self.y, self.core = tp // 2, lax.rem(tp, 2)

    def device(self, z=0, x=0, y=0, core=0):
        fs = around(self.z + z) * SIDE + around(self.x + x)
        tp = around(self.y + y) * 2 + lax.rem(self.core + core, 2)
        return (fs, tp)

    def neighbours(self):
        return [self.device(**{a: d}) for a in ("z", "x", "y") for d in (1, -1)] + [
            self.device(core=1)
        ]


def remote(src, dst, device, send, receive):
    return pltpu.make_async_remote_copy(
        src_ref=src, dst_ref=dst, send_sem=send, recv_sem=receive, device_id=device, device_id_type=MESH
    )


class Ring:
    def __init__(self, place, parts, half, bulk, sems, bases, joint=False, shared=None):
        self.place, self.count, self.bulk, self.sems = place, half * len(parts), bulk, sems
        self.base = bases.pop(0)
        self.side = bases.pop(0) if shared is None else shared
        self.last = self.side if joint else bases.pop(0)
        self.sent = []
        for axis, piece in parts:
            at = getattr(place, axis)
            on, back = place.device(**{axis: 1}), place.device(**{axis: -1})
            before, after = around(at - 1), around(at + 1)
            self.sent.append([
                (piece(at, 0), on),
                (piece(at, 1), on),
                (piece(at, 1), back),
                (piece(at, 0), back),
                (piece(before, 0), on),
                (piece(after, 1), back),
            ])

    def start(self, *which):
        send, receive = self.sems
        for part in self.sent:
            for j in which:
                ref, device = part[j]
                k = (self.base, self.side, self.base, self.side, self.last, self.last)[j]
                remote(ref, ref, device, send, receive.at[k]).start()

    def wait(self, k, halves):
        send, receive = self.sems
        ref = self.bulk(halves * self.count)
        remote(ref, ref, self.place.device(core=1), send, receive.at[k]).wait_recv()

    def own(self):
        self.start(0, 2, 1, 3)

    def forward(self):
        self.wait(self.base, 2)
        self.start(4, 5)

    def near(self):
        self.wait(self.side, 2)

    def far(self):
        self.wait(self.last, 2)

    def rest(self, rings=1):
        self.wait(self.side, 4 * rings)


class Partner:
    def __init__(self, place, block, bulk, sems, base, joint):
        self.bulk, self.sems, self.base = bulk, sems, base
        self.keys = (0, 0, 0, 0) if joint else (0, 0, 0, 1)
        self.device = place.device(core=1)
        self.sent = [block(around(place.y + d), place.core) for d in (0, -1, 1, 2)]

    def start(self, *which):
        send, receive = self.sems
        for j in which:
            ref = self.sent[j]
            remote(ref, ref, self.device, send, receive.at[self.base + self.keys[j]]).start()

    def wait(self, k, blocks):
        send, receive = self.sems
        ref = self.bulk(blocks * ROWS * WIDTH)
        remote(ref, ref, self.device, send, receive.at[self.base + k]).wait_recv()


class RingSum:
    def __init__(self, place, parts, half, bulk, sems, base):
        self.place, self.count, self.bulk, self.sems, self.base = place, half * len(parts), bulk, sems, base
        self.mine, self.boxes, self.sent = [], [], []
        for axis, block, far, near in parts:
            at = getattr(place, axis)
            on, back = place.device(**{axis: 1}), place.device(**{axis: -1})
            before, after, across = around(at - 1), around(at + 1), around(at + 2)
            self.mine.append([block(at, s) for s in range(2)])
            self.boxes.append((far, near))
            self.sent.append([
                (block(across, 0), far(0), on),
                (block(across, 1), far(1), back),
                (block(after, 1), near(0, 1), on),
                (block(before, 0), near(1, 0), back),
                (block(after, 0), near(0, 0), on),
                (block(before, 1), near(1, 1), back),
            ])

    def start(self, which, parts=None):
        send, receive = self.sems
        for part in self.sent if parts is None else [self.sent[p] for p in parts]:
            for j in which:
                src, dst, device = part[j]
                remote(src, dst, device, send, receive.at[self.base + (0 if j < 2 else 1)]).start()

    def begin(self, *parts):
        self.start((0, 1, 2, 3), parts or None)

    def wait(self, k, halves):
        send, receive = self.sems
        ref = self.bulk(halves * self.count)
        remote(ref, ref, self.place.device(core=1), send, receive.at[self.base + k]).wait_recv()

    def middle(self):
        self.wait(0, 2)
        for p, (far, near) in enumerate(self.boxes):
            for j in range(2):
                ref = self.sent[p][4 + j][0]
                ref[...] = (ref[...].astype(f32) + far(j)[...].astype(f32)).astype(bf16)
            self.start((4, 5), (p,))

    def arrive(self):
        self.wait(1, 4)

    def total(self, p, s):
        near = self.boxes[p][1]
        return (
            self.mine[p][s][...].astype(f32)
            + near(0, s)[...].astype(f32)
            + near(1, s)[...].astype(f32)
        )

    def finish(self, result=None):
        self.arrive()
        for p, mine in enumerate(self.mine):
            for s in range(2):
                target = mine[s] if result is None else result.at[pl.ds(s * STRIP, STRIP), :]
                target[...] = self.total(p, s).astype(bf16)


def dot(a, b):
    return jnp.dot(a, b, preferred_element_type=f32)


def dot_turned(a, b):
    return lax.dot_general(a, b, contract_last, preferred_element_type=f32)


def layer_kernel(
    factor,
    later_in, earlier_in, cot_in, up_in, down_in, up_run_in, down_run_in,
    later_out_ref, pre, back_out, up_run, down_run,
    act, turned, up, down, first_up, hidden, early_hidden, grad, part, other, up_sum, down_sum,
    far_row, near_row, far_one, near_one, far_two, near_two,
    load_sem, send_sem, ring_recv, pair_recv, sum_recv,
):
    place = Place()
    barrier = pltpu.get_barrier_semaphore()
    for neighbour in place.neighbours():
        pl.semaphore_signal(barrier, inc=1, device_id=neighbour, device_id_type=MESH)

    def act_at(a, y, core, first, count):
        column = pl.multiple_of((y * 2 + core) * WIDTH, WIDTH)
        return act.at[a, pl.ds(first, count), pl.ds(column, WIDTH)]

    def down_at(h, s, first, count):
        return down.at[pl.ds(h * HALF + s * 256, 256), pl.ds(pl.multiple_of(first * 128, 128), count)]

    def bulk(count):
        return act.at[0, pl.ds(0, count // MODEL), :]

    here = place.z * SIDE + place.x
    mine = [act_at(a, place.y, place.core, 0, ROWS) for a in range(3)]
    loads = [
        (up_in.at[:, pl.ds(0, HALF)], up.at[0, place.z, place.x], 0),
        (down_in, down.at[:, pl.ds(pl.multiple_of(here * 128, 128), 128)], 0),
        (earlier_in, mine[0], 1),
        (up_in.at[:, pl.ds(HALF, HALF)], up.at[1, place.z, place.x], 2),
        (cot_in, mine[1], 2),
        (later_in, mine[2], 2),
        (up_run_in, up_run, 2),
        (down_run_in, down_run, 2),
    ]
    for src, dst, k in loads:
        pltpu.make_async_copy(src, dst, load_sem.at[k]).start()

    def loaded(k, count):
        ref = bulk(count)
        pltpu.make_async_copy(ref, ref, load_sem.at[k]).wait()

    bases = list(range(21))
    sems = (send_sem.at[0], ring_recv)
    rows = [
        Ring(
            place, [("y", lambda k, s, a=a: act_at(a, k, place.core, s * STRIP, STRIP))],
            STRIP * WIDTH, bulk, (send_sem.at[2], ring_recv), bases,
        )
        for a in range(3)
    ]
    pairs = [
        Partner(
            place, lambda y, c, a=a: act_at(a, y, c, 0, ROWS), bulk, (send_sem.at[2], pair_recv),
            (0, 1, 3)[a], a != 1,
        )
        for a in range(3)
    ]
    first, second = [], []
    for h in range(2):
        first.append(Ring(
            place,
            [
                ("z", lambda k, s, h=h: up.at[h, k, place.x, pl.ds(s * 64, 64), :]),
                ("x", lambda k, s, h=h: down_at(h, s, place.z * SIDE + k, 128)),
            ],
            64 * HALF, bulk, sems, bases, h == 1,
        ))
    for d in (0, -1, 1, 2):
        z, x = around(place.z + d), around(place.x + d)
        second.append(Ring(
            place,
            [
                ("x", lambda k, s, z=z: up.at[0, z, k, pl.ds(s * 64, 64), :]),
                ("z", lambda k, s, x=x: down_at(0, s, k * SIDE + x, 128)),
            ],
            64 * HALF, bulk, sems, bases, True, second[0].side if second else None,
        ))
    last = Ring(
        place,
        [
            ("x", lambda k, s: up.at[1, :, k, pl.ds(s * 64, 64), :]),
            ("z", lambda k, s: down_at(1, s, k * SIDE, 512)),
        ],
        SIDE * 64 * HALF, bulk, sems, bases, True,
    )

    sums = iter(range(0, 18, 2))
    row_sums = [
        RingSum(
            place,
            [(
                "y", lambda k, s, a=a: part.at[a, place.core, k, pl.ds(s * STRIP, STRIP), :],
                lambda d, a=a: far_row.at[a, d], lambda d, s, a=a: near_row.at[a, d, s],
            )],
            STRIP * WIDTH, bulk, (send_sem.at[3], sum_recv), next(sums),
        )
        for a in range(2)
    ]
    sems = (send_sem.at[1], sum_recv)
    first_sum = RingSum(
        place,
        [
            (
                "z", lambda k, s: down_sum.at[0, k, :, pl.ds(s * 64, 64), :],
                lambda d: far_one.at[1, 0, d], lambda d, s: near_one.at[1, 0, d, s],
            ),
            (
                "x", lambda k, s: up_sum.at[0, :, k, pl.ds(s * 64, 64), :],
                lambda d: far_one.at[0, 0, d], lambda d, s: near_one.at[0, 0, d, s],
            ),
        ],
        SIDE * 64 * HALF, bulk, sems, next(sums),
    )
    lines, second_sums = [], []
    for q in (2, 1, -1, 0):
        z, x = around(place.z + q), around(place.x + q)
        lines.append(RingSum(
            place,
            [
                (
                    "z", lambda k, s, x=x: down_sum.at[1, k, x, pl.ds(s * 64, 64), :],
                    lambda d, x=x: far_one.at[1, 1, d, x], lambda d, s, x=x: near_one.at[1, 1, d, s, x],
                ),
                (
                    "x", lambda k, s, z=z: up_sum.at[1, z, k, pl.ds(s * 64, 64), :],
                    lambda d, z=z: far_one.at[0, 1, d, z], lambda d, s, z=z: near_one.at[0, 1, d, s, z],
                ),
            ],
            64 * HALF, bulk, sems, next(sums),
        ))
    for h in range(2):
        second_sums.append(RingSum(
            place,
            [
                (
                    "x", lambda k, s, h=h: down_sum.at[h, place.z, k, pl.ds(s * 64, 64), :],
                    lambda d, h=h: far_two.at[1, h, d], lambda d, s, h=h: near_two.at[1, h, d, s],
                ),
                (
                    "z", lambda k, s, h=h: up_sum.at[h, k, place.x, pl.ds(s * 64, 64), :],
                    lambda d, h=h: far_two.at[0, h, d], lambda d, s, h=h: near_two.at[0, h, d, s],
                ),
            ],
            64 * HALF, bulk, sems, next(sums),
        ))

    order = [around(place.y + d) for d in (2, 1, -1, 0)]

    def swap(a, i):
        return remote(
            part.at[a, 1 - place.core, order[i]], other.at[a, order[i]], place.device(core=1),
            send_sem.at[3], pair_recv.at[4 + 3 * a + (0, 1, 2, 2)[i]],
        )

    def sent(i, count):
        ref = act.at[:, pl.ds(0, count // (3 * MODEL)), :]
        remote(ref, ref, place.device(core=1), send_sem.at[i], pair_recv.at[0]).wait_send()

    def strip(m):
        return pl.ds(pl.multiple_of(m * STRIP, STRIP), STRIP)

    def columns(h):
        return pl.ds(h * HALF, HALF)

    def turn(a, core, start, stop):
        @pl.loop(start, stop)
        def _(d):
            block = pl.ds(pl.multiple_of((around(place.y + d) * 2 + core) * WIDTH, WIDTH), WIDTH)
            turned[a, block, :] = act[a, :, block].T

    def up_of(h):
        return up[h].reshape(MODEL, HALF)

    def earlier_up(h):
        @pl.loop(0, 2)
        def _(m):
            value = jnp.maximum(dot(act[0, strip(m), :], up_of(h)), 0.0)
            first_up[strip(m), :] = value
            early_hidden[strip(m), columns(h)] = jnp.square(value).astype(bf16)

    def hidden_grad(h):
        @pl.loop(0, 2)
        def _(m):
            value = dot_turned(act[1, strip(m), :], down[columns(h), :])
            grad[strip(m), columns(h)] = (2.0 * first_up[strip(m), :] * value).astype(bf16)

    def weight_grad(a, source, target, h):
        @pl.loop(0, 4)
        def _(n):
            block = pl.ds(pl.multiple_of(n * 512, 512), 512)
            value = dot(turned[a, block, :], source[:, columns(h)])
            target[h, n] = value.astype(bf16).reshape(SIDE, 128, HALF)

    def later_up(h):
        @pl.loop(0, 2)
        def _(m):
            value = dot(act[2, strip(m), :], up_of(h))
            pre[strip(m), columns(h)] = value.astype(bf16)
            hidden[strip(m), columns(h)] = jnp.square(jnp.maximum(value, 0.0)).astype(bf16)

    def keep(a, n, m, value):
        value = value.astype(bf16)
        part[a, 0, n, strip(m), :] = value[:, :WIDTH]
        part[a, 1, n, strip(m), :] = value[:, WIDTH:]

    def later_out(i):
        n = order[i]
        block = pl.ds(pl.multiple_of(n * 512, 512), 512)

        @pl.loop(0, 2)
        def _(m):
            keep(0, n, m, dot(hidden[strip(m), :], down[:, block]))

        swap(0, i).start()

    def input_grad(i):
        n = order[i]

        @pl.loop(0, 2)
        def _(m):
            weight = jnp.concatenate([up[h, n].reshape(512, HALF) for h in range(2)], axis=1)
            keep(1, n, m, dot_turned(grad[strip(m), :], weight))

        swap(1, i).start()

    def join(a, i):
        if i == 2:
            ref = bulk(2 * ROWS * WIDTH)
            remote(ref, ref, place.device(core=1), send_sem.at[3], pair_recv.at[6 + 3 * a]).wait_recv()
        elif i < 2:
            swap(a, i).wait_recv()
        n = order[i]
        part[a, place.core, n] = (
            part[a, place.core, n].astype(f32) + other[a, n].astype(f32)
        ).astype(bf16)
        row_sums[a].start(((0, 1), (2,), (3,), ())[i])

    def add_running(h):
        second_sums[h].arrive()
        for p, run in enumerate((down_run, up_run)):
            for s in range(2):
                at = run.at[pl.ds(s * 64, 64), columns(h)]
                at[...] = at[...] + second_sums[h].total(p, s) * factor

    pl.semaphore_wait(barrier, 7)
    loaded(0, 128 * HALF + HIDDEN * 128)

    first[0].own()
    second[0].own()
    loaded(1, ROWS * WIDTH)
    rows[0].own()
    pairs[0].start(0)
    first[0].forward()
    loaded(2, 128 * HALF + 2 * ROWS * WIDTH + 4 * 128 * HIDDEN)
    first[1].own()
    first[0].near()
    second[1].own()
    second[2].own()
    second[0].forward()
    rows[0].forward()
    rows[1].own()
    pairs[1].start(0)
    first[0].far()
    second[3].own()
    first[1].forward()
    second[1].forward()
    rows[0].near()
    pairs[0].start(1, 2)
    rows[0].far()
    pairs[0].start(3)
    second[2].forward()
    second[3].forward()
    rows[1].forward()
    rows[2].own()
    pairs[2].start(0)
    first[1].rest()
    last.own()
    pairs[0].wait(0, 4)
    turn(0, place.core, -1, 3)
    turn(0, 1 - place.core, -1, 3)
    rows[1].near()
    pairs[1].start(1, 2)
    second[0].rest(4)
    earlier_up(0)
    rows[1].far()
    pairs[1].start(3)
    turn(1, place.core, -1, 3)
    pairs[1].wait(0, 3)
    turn(1, 1 - place.core, -1, 2)
    pairs[1].wait(1, 1)
    turn(1, 1 - place.core, 2, 3)
    rows[2].forward()
    last.forward()
    weight_grad(1, early_hidden, down_sum, 0)
    first_sum.begin(0)
    hidden_grad(0)
    rows[2].near()
    pairs[2].start(1, 2)
    weight_grad(0, grad, up_sum, 0)
    first_sum.begin(1)
    rows[2].far()
    pairs[2].start(3)
    pairs[2].wait(0, 4)
    later_up(0)
    last.rest()
    earlier_up(1)
    hidden_grad(1)
    input_grad(0)
    input_grad(1)
    first_sum.middle()
    weight_grad(1, early_hidden, down_sum, 1)
    for which in ((0, 1), (2, 3)):
        for line in lines[:3]:
            line.start(which, (0,))
    join(1, 0)
    weight_grad(0, grad, up_sum, 1)
    for which in ((0, 1), (2, 3)):
        for line in lines[:3]:
            line.start(which, (1,))
    join(1, 1)
    input_grad(2)
    input_grad(3)
    later_up(1)
    join(1, 2)
    join(1, 3)
    first_sum.finish()
    second_sums[0].start((0, 1))
    row_sums[1].middle()
    later_out(0)
    later_out(1)
    later_out(2)
    join(0, 0)
    for line in lines[:3]:
        line.middle()
    lines[3].start((0, 1))
    second_sums[0].start((2, 3))
    later_out(3)
    join(0, 1)
    join(0, 2)
    join(0, 3)
    lines[0].finish()
    second_sums[1].start((0, 1))
    lines[3].start((2, 3))
    second_sums[0].middle()
    row_sums[1].finish(back_out)
    lines[1].finish()
    lines[2].finish()
    second_sums[1].start((2, 3))
    row_sums[0].middle()
    lines[3].middle()
    second_sums[1].middle()
    add_running(0)
    row_sums[0].finish(later_out_ref)
    lines[3].finish()
    add_running(1)
    sent(0, 120 * 64 * HALF)
    sent(1, 120 * 64 * HALF)
    sent(2, 18 * STRIP * WIDTH + 12 * ROWS * WIDTH)
    sent(3, 12 * STRIP * WIDTH + 8 * ROWS * WIDTH)


def store_kernel(*refs):
    sources, results, sem = refs[:5], refs[5:10], refs[10]
    copies = [
        pltpu.make_async_copy(src, dst, sem.at[i]) for i, (src, dst) in enumerate(zip(sources, results))
    ]
    for i in (1, 3, 4, 0, 2):
        copies[i].start()
    for copy in copies:
        copy.wait()


def on_device(*arrays):
    factor = float(ROWS * 16) ** (-0.5)
    anywhere = pl.BlockSpec(memory_space=pl.ANY)
    inside = pl.BlockSpec(memory_space=pltpu.VMEM)
    kept = [
        ((ROWS, WIDTH), bf16),
        ((ROWS, HIDDEN), bf16),
        ((ROWS, WIDTH), bf16),
        ((128, HIDDEN), f32),
        ((128, HIDDEN), f32),
    ]
    results = pl.pallas_call(
        lambda *refs: layer_kernel(factor, *refs),
        out_shape=tuple(pltpu.VMEM(shape, kind) for shape, kind in kept),
        in_specs=[anywhere] * 7,
        out_specs=(inside,) * 5,
        scratch_shapes=[
            pltpu.VMEM((3, ROWS, MODEL), bf16),
            pltpu.VMEM((2, MODEL, ROWS), bf16),
            pltpu.VMEM((2, SIDE, SIDE, 128, HALF), bf16),
            pltpu.VMEM((HIDDEN, MODEL), bf16),
            pltpu.VMEM((ROWS, HALF), f32),
            pltpu.VMEM((ROWS, HIDDEN), bf16),
            pltpu.VMEM((ROWS, HIDDEN), bf16),
            pltpu.VMEM((ROWS, HIDDEN), bf16),
            pltpu.VMEM((2, 2, SIDE, ROWS, WIDTH), bf16),
            pltpu.VMEM((2, SIDE, ROWS, WIDTH), bf16),
            pltpu.VMEM((2, SIDE, SIDE, 128, HALF), bf16),
            pltpu.VMEM((2, SIDE, SIDE, 128, HALF), bf16),
            pltpu.VMEM((2, 2, STRIP, WIDTH), bf16),
            pltpu.VMEM((2, 2, 2, STRIP, WIDTH), bf16),
            pltpu.VMEM((2, 2, 2, SIDE, 64, HALF), bf16),
            pltpu.VMEM((2, 2, 2, 2, SIDE, 64, HALF), bf16),
            pltpu.VMEM((2, 2, 2, 64, HALF), bf16),
            pltpu.VMEM((2, 2, 2, 2, 64, HALF), bf16),
            pltpu.SemaphoreType.DMA((3,)),
            pltpu.SemaphoreType.DMA((4,)),
            pltpu.SemaphoreType.DMA((21,)),
            pltpu.SemaphoreType.DMA((10,)),
            pltpu.SemaphoreType.DMA((18,)),
        ],
        compiler_params=pltpu.CompilerParams(
            collective_id=0, has_side_effects=True, vmem_limit_bytes=LIMIT
        ),
    )(*arrays)
    return pl.pallas_call(
        store_kernel,
        out_shape=tuple(jax.ShapeDtypeStruct(shape, kind) for shape, kind in kept),
        in_specs=[inside] * 5,
        out_specs=(anywhere,) * 5,
        scratch_shapes=[pltpu.SemaphoreType.DMA((5,))],
        compiler_params=pltpu.CompilerParams(vmem_limit_bytes=2**20),
    )(*[pltpu.with_memory_space_constraint(r, pltpu.VMEM) for r in results])


def solution(mesh):
    in_specs = (
        P("fs", "tp"),
        P("fs", "tp"),
        P("fs", "tp"),
        P("fs", "tp"),
        P("tp", "fs"),
        P("fs", "tp"),
        P("fs", "tp"),
    )
    out_specs = (P("fs", "tp"),) * 5
    return jax.shard_map(
        on_device, mesh=mesh, in_specs=in_specs, out_specs=out_specs, check_vma=False
    )
```

```python
import jax
import jax.numpy as jnp
from jax import lax
from jax.experimental import pallas as pl
from jax.experimental.pallas import tpu as pltpu
from jax.sharding import PartitionSpec as P

contract_last = (((1,), (1,)), ((), ()))
bf16, f32 = jnp.bfloat16, jnp.float32
MESH = pl.DeviceIdType.MESH
SIDE = 4
ROWS, WIDTH, MODEL, HIDDEN = 768, 256, 2048, 1024
HALF = HIDDEN // 2
STRIP = ROWS // 2
LIMIT = 60 * 2**20


def around(k):
    return lax.rem(k + SIDE, SIDE)


class Place:
    def __init__(self):
        fs, tp = lax.axis_index("fs"), lax.axis_index("tp")
        self.z, self.x = fs // SIDE, lax.rem(fs, SIDE)
        self.y, self.core = tp // 2, lax.rem(tp, 2)

    def device(self, z=0, x=0, y=0, core=0):
        fs = around(self.z + z) * SIDE + around(self.x + x)
        tp = around(self.y + y) * 2 + lax.rem(self.core + core, 2)
        return (fs, tp)

    def neighbours(self):
        return [self.device(**{a: d}) for a in ("z", "x", "y") for d in (1, -1)] + [
            self.device(core=1)
        ]


def remote(src, dst, device, send, receive):
    return pltpu.make_async_remote_copy(
        src_ref=src, dst_ref=dst, send_sem=send, recv_sem=receive, device_id=device, device_id_type=MESH
    )


class Ring:
    def __init__(self, place, parts, half, bulk, sems, bases, joint=False, shared=None):
        self.place, self.count, self.bulk, self.sems = place, half * len(parts), bulk, sems
        self.base = bases.pop(0)
        self.side = bases.pop(0) if shared is None else shared
        self.last = self.side if joint else bases.pop(0)
        self.sent = []
        for axis, piece in parts:
            at = getattr(place, axis)
            on, back = place.device(**{axis: 1}), place.device(**{axis: -1})
            before, after = around(at - 1), around(at + 1)
            self.sent.append([
                (piece(at, 0), on),
                (piece(at, 1), on),
                (piece(at, 1), back),
                (piece(at, 0), back),
                (piece(before, 0), on),
                (piece(after, 1), back),
            ])

    def start(self, *which):
        send, receive = self.sems
        for part in self.sent:
            for j in which:
                ref, device = part[j]
                k = (self.base, self.side, self.base, self.side, self.last, self.last)[j]
                remote(ref, ref, device, send, receive.at[k]).start()

    def wait(self, k, halves):
        send, receive = self.sems
        ref = self.bulk(halves * self.count)
        remote(ref, ref, self.place.device(core=1), send, receive.at[k]).wait_recv()

    def own(self):
        self.start(0, 2, 1, 3)

    def forward(self):
        self.wait(self.base, 2)
        self.start(4, 5)

    def near(self):
        self.wait(self.side, 2)

    def far(self):
        self.wait(self.last, 2)

    def rest(self, rings=1):
        self.wait(self.side, 4 * rings)


class Partner:
    def __init__(self, place, block, bulk, sems, base, joint):
        self.bulk, self.sems, self.base = bulk, sems, base
        self.keys = (0, 0, 0, 0) if joint else (0, 0, 0, 1)
        self.device = place.device(core=1)
        self.sent = [block(around(place.y + d), place.core) for d in (0, -1, 1, 2)]

    def start(self, *which):
        send, receive = self.sems
        for j in which:
            ref = self.sent[j]
            remote(ref, ref, self.device, send, receive.at[self.base + self.keys[j]]).start()

    def wait(self, k, blocks):
        send, receive = self.sems
        ref = self.bulk(blocks * ROWS * WIDTH)
        remote(ref, ref, self.device, send, receive.at[self.base + k]).wait_recv()


class RingSum:
    def __init__(self, place, parts, half, bulk, sems, base):
        self.place, self.count, self.bulk, self.sems, self.base = place, half * len(parts), bulk, sems, base
        self.mine, self.boxes, self.sent = [], [], []
        for axis, block, far, near in parts:
            at = getattr(place, axis)
            on, back = place.device(**{axis: 1}), place.device(**{axis: -1})
            before, after, across = around(at - 1), around(at + 1), around(at + 2)
            self.mine.append([block(at, s) for s in range(2)])
            self.boxes.append((far, near))
            self.sent.append([
                (block(across, 0), far(0), on),
                (block(across, 1), far(1), back),
                (block(after, 1), near(0, 1), on),
                (block(before, 0), near(1, 0), back),
                (block(after, 0), near(0, 0), on),
                (block(before, 1), near(1, 1), back),
            ])

    def start(self, which, parts=None):
        send, receive = self.sems
        for part in self.sent if parts is None else [self.sent[p] for p in parts]:
            for j in which:
                src, dst, device = part[j]
                remote(src, dst, device, send, receive.at[self.base + (0 if j < 2 else 1)]).start()

    def begin(self, *parts):
        self.start((0, 1, 2, 3), parts or None)

    def wait(self, k, halves):
        send, receive = self.sems
        ref = self.bulk(halves * self.count)
        remote(ref, ref, self.place.device(core=1), send, receive.at[self.base + k]).wait_recv()

    def middle(self):
        self.wait(0, 2)
        for p, (far, near) in enumerate(self.boxes):
            for j in range(2):
                ref = self.sent[p][4 + j][0]
                ref[...] = (ref[...].astype(f32) + far(j)[...].astype(f32)).astype(bf16)
            self.start((4, 5), (p,))

    def arrive(self):
        self.wait(1, 4)

    def total(self, p, s):
        near = self.boxes[p][1]
        return (
            self.mine[p][s][...].astype(f32)
            + near(0, s)[...].astype(f32)
            + near(1, s)[...].astype(f32)
        )

    def finish(self, result=None):
        self.arrive()
        for p, mine in enumerate(self.mine):
            for s in range(2):
                target = mine[s] if result is None else result.at[pl.ds(s * STRIP, STRIP), :]
                target[...] = self.total(p, s).astype(bf16)


def dot(a, b):
    return jnp.dot(a, b, preferred_element_type=f32)


def dot_turned(a, b):
    return lax.dot_general(a, b, contract_last, preferred_element_type=f32)


def layer_kernel(
    factor,
    later_in, earlier_in, cot_in, up_in, down_in, up_run_in, down_run_in,
    later_out_ref, pre, back_out, up_run, down_run,
    act, turned, up, down, first_up, hidden, early_hidden, grad, part, other, up_sum, down_sum,
    far_row, near_row, far_one, near_one, far_two, near_two,
    load_sem, send_sem, ring_recv, pair_recv, sum_recv,
):
    place = Place()
    barrier = pltpu.get_barrier_semaphore()
    for neighbour in place.neighbours():
        pl.semaphore_signal(barrier, inc=1, device_id=neighbour, device_id_type=MESH)

    def act_at(a, y, core, first, count):
        column = pl.multiple_of((y * 2 + core) * WIDTH, WIDTH)
        return act.at[a, pl.ds(first, count), pl.ds(column, WIDTH)]

    def down_at(h, s, first, count):
        return down.at[pl.ds(h * HALF + s * 256, 256), pl.ds(pl.multiple_of(first * 128, 128), count)]

    def bulk(count):
        return act.at[0, pl.ds(0, count // MODEL), :]

    here = place.z * SIDE + place.x
    mine = [act_at(a, place.y, place.core, 0, ROWS) for a in range(3)]
    loads = [
        (up_in.at[:, pl.ds(0, HALF)], up.at[0, place.z, place.x], 0),
        (down_in, down.at[:, pl.ds(pl.multiple_of(here * 128, 128), 128)], 0),
        (earlier_in, mine[0], 1),
        (up_in.at[:, pl.ds(HALF, HALF)], up.at[1, place.z, place.x], 2),
        (cot_in, mine[1], 2),
        (later_in, mine[2], 2),
        (up_run_in, up_run, 2),
        (down_run_in, down_run, 2),
    ]
    for src, dst, k in loads:
        pltpu.make_async_copy(src, dst, load_sem.at[k]).start()

    def loaded(k, count):
        ref = bulk(count)
        pltpu.make_async_copy(ref, ref, load_sem.at[k]).wait()

    bases = list(range(21))
    sems = (send_sem.at[0], ring_recv)
    rows = [
        Ring(
            place, [("y", lambda k, s, a=a: act_at(a, k, place.core, s * STRIP, STRIP))],
            STRIP * WIDTH, bulk, (send_sem.at[2], ring_recv), bases,
        )
        for a in range(3)
    ]
    pairs = [
        Partner(
            place, lambda y, c, a=a: act_at(a, y, c, 0, ROWS), bulk, (send_sem.at[2], pair_recv),
            (0, 1, 3)[a], a != 1,
        )
        for a in range(3)
    ]
    first, second = [], []
    for h in range(2):
        first.append(Ring(
            place,
            [
                ("z", lambda k, s, h=h: up.at[h, k, place.x, pl.ds(s * 64, 64), :]),
                ("x", lambda k, s, h=h: down_at(h, s, place.z * SIDE + k, 128)),
            ],
            64 * HALF, bulk, sems, bases, h == 1,
        ))
    for d in (0, -1, 1, 2):
        z, x = around(place.z + d), around(place.x + d)
        second.append(Ring(
            place,
            [
                ("x", lambda k, s, z=z: up.at[0, z, k, pl.ds(s * 64, 64), :]),
                ("z", lambda k, s, x=x: down_at(0, s, k * SIDE + x, 128)),
            ],
            64 * HALF, bulk, sems, bases, True, second[0].side if second else None,
        ))
    last = Ring(
        place,
        [
            ("x", lambda k, s: up.at[1, :, k, pl.ds(s * 64, 64), :]),
            ("z", lambda k, s: down_at(1, s, k * SIDE, 512)),
        ],
        SIDE * 64 * HALF, bulk, sems, bases, True,
    )

    sums = iter(range(0, 18, 2))
    row_sums = [
        RingSum(
            place,
            [(
                "y", lambda k, s, a=a: part.at[a, place.core, k, pl.ds(s * STRIP, STRIP), :],
                lambda d, a=a: far_row.at[a, d], lambda d, s, a=a: near_row.at[a, d, s],
            )],
            STRIP * WIDTH, bulk, (send_sem.at[3], sum_recv), next(sums),
        )
        for a in range(2)
    ]
    sems = (send_sem.at[1], sum_recv)
    first_sum = RingSum(
        place,
        [
            (
                "z", lambda k, s: down_sum.at[0, k, :, pl.ds(s * 64, 64), :],
                lambda d: far_one.at[1, 0, d], lambda d, s: near_one.at[1, 0, d, s],
            ),
            (
                "x", lambda k, s: up_sum.at[0, :, k, pl.ds(s * 64, 64), :],
                lambda d: far_one.at[0, 0, d], lambda d, s: near_one.at[0, 0, d, s],
            ),
        ],
        SIDE * 64 * HALF, bulk, sems, next(sums),
    )
    lines, second_sums = [], []
    for q in (2, 1, -1, 0):
        z, x = around(place.z + q), around(place.x + q)
        lines.append(RingSum(
            place,
            [
                (
                    "z", lambda k, s, x=x: down_sum.at[1, k, x, pl.ds(s * 64, 64), :],
                    lambda d, x=x: far_one.at[1, 1, d, x], lambda d, s, x=x: near_one.at[1, 1, d, s, x],
                ),
                (
                    "x", lambda k, s, z=z: up_sum.at[1, z, k, pl.ds(s * 64, 64), :],
                    lambda d, z=z: far_one.at[0, 1, d, z], lambda d, s, z=z: near_one.at[0, 1, d, s, z],
                ),
            ],
            64 * HALF, bulk, sems, next(sums),
        ))
    for h in range(2):
        second_sums.append(RingSum(
            place,
            [
                (
                    "x", lambda k, s, h=h: down_sum.at[h, place.z, k, pl.ds(s * 64, 64), :],
                    lambda d, h=h: far_two.at[1, h, d], lambda d, s, h=h: near_two.at[1, h, d, s],
                ),
                (
                    "z", lambda k, s, h=h: up_sum.at[h, k, place.x, pl.ds(s * 64, 64), :],
                    lambda d, h=h: far_two.at[0, h, d], lambda d, s, h=h: near_two.at[0, h, d, s],
                ),
            ],
            64 * HALF, bulk, sems, next(sums),
        ))

    order = [around(place.y + d) for d in (2, 1, -1, 0)]

    def swap(a, i):
        return remote(
            part.at[a, 1 - place.core, order[i]], other.at[a, order[i]], place.device(core=1),
            send_sem.at[3], pair_recv.at[4 + 3 * a + (0, 1, 2, 2)[i]],
        )

    def sent(i, count):
        ref = act.at[:, pl.ds(0, count // (3 * MODEL)), :]
        remote(ref, ref, place.device(core=1), send_sem.at[i], pair_recv.at[0]).wait_send()

    def strip(m):
        return pl.ds(pl.multiple_of(m * STRIP, STRIP), STRIP)

    def columns(h):
        return pl.ds(h * HALF, HALF)

    def turn(a, core, start, stop):
        @pl.loop(start, stop)
        def _(d):
            block = pl.ds(pl.multiple_of((around(place.y + d) * 2 + core) * WIDTH, WIDTH), WIDTH)
            turned[a, block, :] = act[a, :, block].T

    def up_of(h):
        return up[h].reshape(MODEL, HALF)

    def earlier_up(h):
        @pl.loop(0, 2)
        def _(m):
            value = jnp.maximum(dot(act[0, strip(m), :], up_of(h)), 0.0)
            first_up[strip(m), :] = value
            early_hidden[strip(m), columns(h)] = jnp.square(value).astype(bf16)

    def hidden_grad(h):
        @pl.loop(0, 2)
        def _(m):
            value = dot_turned(act[1, strip(m), :], down[columns(h), :])
            grad[strip(m), columns(h)] = (2.0 * first_up[strip(m), :] * value).astype(bf16)

    def weight_grad(a, source, target, h):
        @pl.loop(0, 4)
        def _(n):
            block = pl.ds(pl.multiple_of(n * 512, 512), 512)
            value = dot(turned[a, block, :], source[:, columns(h)])
            target[h, n] = value.astype(bf16).reshape(SIDE, 128, HALF)

    def later_up(h):
        @pl.loop(0, 2)
        def _(m):
            value = dot(act[2, strip(m), :], up_of(h))
            pre[strip(m), columns(h)] = value.astype(bf16)
            hidden[strip(m), columns(h)] = jnp.square(jnp.maximum(value, 0.0)).astype(bf16)

    def keep(a, n, m, value):
        value = value.astype(bf16)
        part[a, 0, n, strip(m), :] = value[:, :WIDTH]
        part[a, 1, n, strip(m), :] = value[:, WIDTH:]

    def later_out(i):
        n = order[i]
        block = pl.ds(pl.multiple_of(n * 512, 512), 512)

        @pl.loop(0, 2)
        def _(m):
            keep(0, n, m, dot(hidden[strip(m), :], down[:, block]))

        swap(0, i).start()

    def input_grad(i):
        n = order[i]

        @pl.loop(0, 2)
        def _(m):
            weight = jnp.concatenate([up[h, n].reshape(512, HALF) for h in range(2)], axis=1)
            keep(1, n, m, dot_turned(grad[strip(m), :], weight))

        swap(1, i).start()

    def join(a, i):
        if i == 2:
            ref = bulk(2 * ROWS * WIDTH)
            remote(ref, ref, place.device(core=1), send_sem.at[3], pair_recv.at[6 + 3 * a]).wait_recv()
        elif i < 2:
            swap(a, i).wait_recv()
        n = order[i]
        part[a, place.core, n] = (
            part[a, place.core, n].astype(f32) + other[a, n].astype(f32)
        ).astype(bf16)
        row_sums[a].start(((0, 1), (2,), (3,), ())[i])

    def add_running(h):
        second_sums[h].arrive()
        for p, run in enumerate((down_run, up_run)):
            for s in range(2):
                at = run.at[pl.ds(s * 64, 64), columns(h)]
                at[...] = at[...] + second_sums[h].total(p, s) * factor

    pl.semaphore_wait(barrier, 7)
    loaded(0, 128 * HALF + HIDDEN * 128)

    first[0].own()
    second[0].own()
    loaded(1, ROWS * WIDTH)
    rows[0].own()
    pairs[0].start(0)
    first[0].forward()
    loaded(2, 128 * HALF + 2 * ROWS * WIDTH + 4 * 128 * HIDDEN)
    first[1].own()
    first[0].near()
    second[1].own()
    second[2].own()
    second[0].forward()
    rows[0].forward()
    rows[1].own()
    pairs[1].start(0)
    first[0].far()
    second[3].own()
    first[1].forward()
    second[1].forward()
    rows[0].near()
    pairs[0].start(1, 2)
    rows[0].far()
    pairs[0].start(3)
    second[2].forward()
    second[3].forward()
    rows[1].forward()
    rows[2].own()
    pairs[2].start(0)
    first[1].rest()
    last.own()
    pairs[0].wait(0, 4)
    turn(0, place.core, -1, 3)
    turn(0, 1 - place.core, -1, 3)
    rows[1].near()
    pairs[1].start(1, 2)
    second[0].rest(4)
    earlier_up(0)
    rows[1].far()
    pairs[1].start(3)
    turn(1, place.core, -1, 3)
    pairs[1].wait(0, 3)
    turn(1, 1 - place.core, -1, 2)
    pairs[1].wait(1, 1)
    turn(1, 1 - place.core, 2, 3)
    rows[2].forward()
    last.forward()
    weight_grad(1, early_hidden, down_sum, 0)
    first_sum.begin(0)
    hidden_grad(0)
    rows[2].near()
    pairs[2].start(1, 2)
    weight_grad(0, grad, up_sum, 0)
    first_sum.begin(1)
    rows[2].far()
    pairs[2].start(3)
    pairs[2].wait(0, 4)
    later_up(0)
    last.rest()
    earlier_up(1)
    hidden_grad(1)
    input_grad(0)
    input_grad(1)
    first_sum.middle()
    weight_grad(1, early_hidden, down_sum, 1)
    for which in ((0, 1), (2, 3)):
        for line in lines[:3]:
            line.start(which, (0,))
    join(1, 0)
    weight_grad(0, grad, up_sum, 1)
    for which in ((0, 1), (2, 3)):
        for line in lines[:3]:
            line.start(which, (1,))
    join(1, 1)
    input_grad(2)
    input_grad(3)
    later_up(1)
    join(1, 2)
    join(1, 3)
    first_sum.finish()
    second_sums[0].start((0, 1))
    row_sums[1].middle()
    later_out(0)
    later_out(1)
    later_out(2)
    join(0, 0)
    for line in lines[:3]:
        line.middle()
    lines[3].start((0, 1))
    second_sums[0].start((2, 3))
    later_out(3)
    join(0, 1)
    join(0, 2)
    join(0, 3)
    lines[0].finish()
    second_sums[1].start((0, 1))
    second_sums[0].middle()
    row_sums[1].finish(back_out)
    lines[1].finish()
    lines[2].finish()
    lines[3].start((2, 3))
    second_sums[1].start((2, 3))
    lines[3].middle()
    row_sums[0].middle()
    second_sums[1].middle()
    add_running(0)
    row_sums[0].finish(later_out_ref)
    lines[3].finish()
    add_running(1)
    sent(0, 120 * 64 * HALF)
    sent(1, 120 * 64 * HALF)
    sent(2, 18 * STRIP * WIDTH + 12 * ROWS * WIDTH)
    sent(3, 12 * STRIP * WIDTH + 8 * ROWS * WIDTH)


def store_kernel(*refs):
    sources, results, sem = refs[:5], refs[5:10], refs[10]
    copies = [
        pltpu.make_async_copy(src, dst, sem.at[i]) for i, (src, dst) in enumerate(zip(sources, results))
    ]
    for i in (1, 3, 4, 0, 2):
        copies[i].start()
    for copy in copies:
        copy.wait()


def on_device(*arrays):
    factor = float(ROWS * 16) ** (-0.5)
    anywhere = pl.BlockSpec(memory_space=pl.ANY)
    inside = pl.BlockSpec(memory_space=pltpu.VMEM)
    kept = [
        ((ROWS, WIDTH), bf16),
        ((ROWS, HIDDEN), bf16),
        ((ROWS, WIDTH), bf16),
        ((128, HIDDEN), f32),
        ((128, HIDDEN), f32),
    ]
    results = pl.pallas_call(
        lambda *refs: layer_kernel(factor, *refs),
        out_shape=tuple(pltpu.VMEM(shape, kind) for shape, kind in kept),
        in_specs=[anywhere] * 7,
        out_specs=(inside,) * 5,
        scratch_shapes=[
            pltpu.VMEM((3, ROWS, MODEL), bf16),
            pltpu.VMEM((2, MODEL, ROWS), bf16),
            pltpu.VMEM((2, SIDE, SIDE, 128, HALF), bf16),
            pltpu.VMEM((HIDDEN, MODEL), bf16),
            pltpu.VMEM((ROWS, HALF), f32),
            pltpu.VMEM((ROWS, HIDDEN), bf16),
            pltpu.VMEM((ROWS, HIDDEN), bf16),
            pltpu.VMEM((ROWS, HIDDEN), bf16),
            pltpu.VMEM((2, 2, SIDE, ROWS, WIDTH), bf16),
            pltpu.VMEM((2, SIDE, ROWS, WIDTH), bf16),
            pltpu.VMEM((2, SIDE, SIDE, 128, HALF), bf16),
            pltpu.VMEM((2, SIDE, SIDE, 128, HALF), bf16),
            pltpu.VMEM((2, 2, STRIP, WIDTH), bf16),
            pltpu.VMEM((2, 2, 2, STRIP, WIDTH), bf16),
            pltpu.VMEM((2, 2, 2, SIDE, 64, HALF), bf16),
            pltpu.VMEM((2, 2, 2, 2, SIDE, 64, HALF), bf16),
            pltpu.VMEM((2, 2, 2, 64, HALF), bf16),
            pltpu.VMEM((2, 2, 2, 2, 64, HALF), bf16),
            pltpu.SemaphoreType.DMA((3,)),
            pltpu.SemaphoreType.DMA((4,)),
            pltpu.SemaphoreType.DMA((21,)),
            pltpu.SemaphoreType.DMA((10,)),
            pltpu.SemaphoreType.DMA((18,)),
        ],
        compiler_params=pltpu.CompilerParams(
            collective_id=0, has_side_effects=True, vmem_limit_bytes=LIMIT
        ),
    )(*arrays)
    return pl.pallas_call(
        store_kernel,
        out_shape=tuple(jax.ShapeDtypeStruct(shape, kind) for shape, kind in kept),
        in_specs=[inside] * 5,
        out_specs=(anywhere,) * 5,
        scratch_shapes=[pltpu.SemaphoreType.DMA((5,))],
        compiler_params=pltpu.CompilerParams(vmem_limit_bytes=2**20),
    )(*[pltpu.with_memory_space_constraint(r, pltpu.VMEM) for r in results])


def solution(mesh):
    in_specs = (
        P("fs", "tp"),
        P("fs", "tp"),
        P("fs", "tp"),
        P("fs", "tp"),
        P("tp", "fs"),
        P("fs", "tp"),
        P("fs", "tp"),
    )
    out_specs = (P("fs", "tp"),) * 5
    return jax.shard_map(
        on_device, mesh=mesh, in_specs=in_specs, out_specs=out_specs, check_vma=False
    )
```
